256 devices in a mesh: ep: 64 (over z, x, core), tp: 4 (over y).
Axes of the slice: x: 4, y: 4, z: 8, core: 2. Of those that a mesh axis runs over, the one named last changes fastest.
Arguments:
- layer_in: bfloat16 [1024, 2048], P('ep'), may hold values from -6 to 6
- state_in: float32 [1024, 32, 4096], P('ep', 'tp'), may hold values from -6 to 6
- mix_gain: float32 [2048], replicated, may hold values from 0.1 to 1.9
- rec_weight: bfloat16 [2048, 2048], P('ep', 'tp'), may hold values from -0.125 to 0.125
- key_weight: bfloat16 [2048, 2048], P('ep', 'tp'), may hold values from -0.125 to 0.125
- val_weight: bfloat16 [2048, 2048], P('ep', 'tp'), may hold values from -0.125 to 0.125
- decay_down: bfloat16 [2048, 64], replicated, may hold values from -0.125 to 0.125
- decay_up: bfloat16 [64, 2048], P(None, 'tp'), may hold values from -0.75 to 0.75
- decay_base: float32 [2048], P('tp'), may hold values from -6 to 6
- rate_down: bfloat16 [2048, 64], replicated, may hold values from -0.125 to 0.125
- rate_up: bfloat16 [64, 2048], P(None, 'tp'), may hold values from -0.75 to 0.75
- rate_base: float32 [2048], P('tp'), may hold values from -6 to 6
- key_scale: float32 [2048], P('tp'), may hold values from 0.25 to 4
- group_gain: float32 [2048], P('tp'), may hold values from 0.1 to 1.9
- out_weight: bfloat16 [2048, 2048], P('tp', 'ep'), may hold values from -0.125 to 0.125
- post_gain: float32 [2048], replicated, may hold values from 0.1 to 1.9
- ffn_gain: float32 [2048], replicated, may hold values from 0.1 to 1.9
- routes: int32 [1024, 4], P('ep'), may hold values from 0 to 63, all different within a row; in each aligned block of 16 rows (0 to 15, 16 to 31, ...) at most 2 rows name the same one
- route_gates: float32 [1024, 4], P('ep'), may hold values from 0.05 to 1
- expert_gate: bfloat16 [64, 2048, 2048], P('ep', None, 'tp'), may hold values from -0.375 to 0.375
- expert_up: bfloat16 [64, 2048, 2048], P('ep', None, 'tp'), may hold values from -0.375 to 0.375
- expert_down: bfloat16 [64, 2048, 2048], P('ep', 'tp'), may hold values from -0.125 to 0.125
- out_gain: float32 [2048], replicated, may hold values from 0.1 to 1.9
Outputs:
- layer_out: bfloat16 [1024, 2048], P('ep')
- new_state: float32 [1024, 32, 4096], P('ep', 'tp')
The draws below stay inside these ranges and needn't reach their ends.
Inputs may be any that keep to these rules, and one draw needn't show every extreme that they name: `routes`: each row names 4 different experts. Within the rows of one device (aligned blocks of 16 rows) no expert is named by more than 2 rows, and in every draw some block names some expert exactly 2 times.
All inputs are finite; a program needn't handle non-finite values.
Results may differ from the reference program's by a relative error of at most 0.017.
Values may be sent and summed in bfloat16 or wider, within the bound.
A program may use at most 128 MiB of HBM per device.

```python
import math
import jax
import jax.numpy as jnp
import numpy as np
from jax import lax

D = 2048
HEADS = 32
HEAD_DIM = 64
LOW = 64
FF = 2048
TOPK = 4
SEQ_DEV = 16
SEQS = 1024
EXPERTS = 64
CAP = 2
N_EP = 64
N_TP = 4


def shard_levels(stream_key, shape, pieces, smallest, largest):
    def one(position, blocks):
        steps = jax.random.uniform(jax.random.fold_in(jax.random.fold_in(stream_key, 6), position), (blocks,), jnp.float32, smallest / len(pieces), largest / len(pieces))
        return jnp.repeat(jnp.exp(steps), shape[position] // blocks).reshape((-1,) + (1,) * (len(shape) - position - 1))

    factor_of = one(*pieces[0])
    for cut in pieces[1:]:
        factor_of = factor_of * one(*cut)
    return factor_of


def routed_block(own_key, own, number, rows, amount, top, limit, slope):
    ranking = jax.random.permutation(own_key, amount)
    packed, common = shares(amount, rows * top, limit, slope, True), shares(amount, rows * top, limit, slope, False)
    places = jnp.arange(amount)

    def named(sizes, turn):
        used = int((sizes > 0).sum())
        fixed = max(1, used // 4)
        moved = fixed + (places - fixed + turn * (used - fixed)) % max(1, amount - fixed)
        return jnp.zeros((amount,), jnp.int32).at[ranking[jnp.where(places < fixed, places, moved)]].set(jnp.asarray(sizes, jnp.int32))

    sizes = jnp.where(number % 4 == 0, named(packed, number // 4), named(common, number - number // 4 - 1))
    mixed = jax.random.permutation(jax.random.fold_in(own, 3), amount)
    donor, taker = mixed[0:amount // 2 * 2:2], mixed[1:amount // 2 * 2:2]
    margin = jnp.minimum(sizes[donor] - 1, limit - sizes[taker]) // 2
    margin = jnp.where((donor == ranking[0]) | (taker == ranking[0]) | (sizes[taker] == 0), 0, jnp.maximum(margin, 0))
    moved = jax.random.randint(jax.random.fold_in(own, 4), (amount // 2,), 0, 1 << 20) % (margin + 1)
    sizes = sizes.at[donor].add(-moved).at[taker].add(moved)
    items = jnp.searchsorted(jnp.cumsum(sizes), jnp.arange(rows * top), side="right").astype(jnp.int32)
    grid = items.reshape(top, rows).T
    grid = grid[jax.random.permutation(jax.random.fold_in(own, 1), rows)]
    turn = jax.random.randint(jax.random.fold_in(own, 2), (rows, 1), 0, top)
    return jnp.take_along_axis(grid, (jnp.arange(top)[None, :] + turn) % top, axis=1)


def shares(number_of, total, most, slope, full):
    loads = [(1 << 20) // math.isqrt(grade ** slope) + 1 for grade in range(1, number_of + 1)]
    largest = most if full else min(most, max(-(-total // number_of), total * loads[0] // sum(loads)))
    least = 1 if total - largest >= number_of - 1 else 0
    counts, rest = [largest] + [least] * (number_of - 1), total - largest - least * (number_of - 1)
    while rest > 0:
        candidates = [i for i in range(1, number_of) if counts[i] < largest] or [i for i in range(1, number_of) if counts[i] < most]
        mass, budget = sum([loads[i] for i in candidates]), rest
        for i in candidates:
            extra = min(most - counts[i], max(1, budget * loads[i] // mass), rest)
            counts[i] = counts[i] + extra
            rest = rest - extra
    return np.array(counts)


def bell_draw(stream_key, extent, spread, limit, shards=(), kind=jnp.bfloat16):
    entries = jax.random.normal(stream_key, extent, jnp.float32) * spread
    if len(shards) > 0:
        entries = shard_levels(stream_key, extent, shards, -0.22, 0.18) * entries
    return jnp.clip(entries, min=-limit, max=limit).astype(kind)


def setup_inputs(seed: int = 0) -> dict:
    seeds = jax.random.split(jax.random.key(seed), 24)
    layer_in = bell_draw(seeds[0], (SEQS, D), 1.0, 6.0, ((0, 64),))
    state_in = bell_draw(seeds[1], (SEQS, HEADS, HEAD_DIM * HEAD_DIM), 1.0, 6.0, ((0, 64), (1, 4)), jnp.float32)
    mix_gain = jnp.clip(1.0 + 0.18 * jax.random.normal(seeds[2], (D,), jnp.float32), 0.1, 1.9)
    rec_weight = bell_draw(seeds[3], (D, D), D ** -0.5, 0.125, ((0, 64), (1, 4)))
    key_weight = bell_draw(seeds[4], (D, D), D ** -0.5, 0.125, ((0, 64), (1, 4)))
    val_weight = bell_draw(seeds[5], (D, D), D ** -0.5, 0.125, ((0, 64), (1, 4)))
    decay_down = bell_draw(seeds[6], (D, LOW), D ** -0.5, 0.125)
    decay_up = bell_draw(seeds[7], (LOW, D), LOW ** -0.5, 0.75, ((1, 4),))
    decay_base = bell_draw(seeds[8], (D,), 1.5, 6.0, ((0, 4),), jnp.float32)
    rate_down = bell_draw(seeds[9], (D, LOW), D ** -0.5, 0.125)
    rate_up = bell_draw(seeds[10], (LOW, D), LOW ** -0.5, 0.75, ((1, 4),))
    rate_base = bell_draw(seeds[11], (D,), 1.0, 6.0, ((0, 4),), jnp.float32)
    key_scale = jnp.clip(jnp.exp(math.log(4.0) - 2.7725887 * jax.random.uniform(seeds[12], (D,), jnp.float32) ** shard_levels(seeds[12], (D,), ((0, 4),), -0.2, 0.2)), 0.25, 4.0)
    group_gain = jnp.clip(1.0 + 0.18 * jax.random.normal(seeds[13], (D,), jnp.float32), 0.1, 1.9)
    out_weight = bell_draw(seeds[14], (D, D), D ** -0.5, 0.125, ((0, 4), (1, 64)))
    post_gain = jnp.clip(1.0 + 0.18 * jax.random.normal(seeds[15], (D,), jnp.float32), 0.1, 1.9)
    ffn_gain = jnp.clip(1.0 + 0.18 * jax.random.normal(seeds[16], (D,), jnp.float32), 0.1, 1.9)
    routes_keys = jax.random.split(jax.random.fold_in(seeds[17], 1), SEQS // SEQ_DEV)
    routes_turns = jax.random.permutation(jax.random.fold_in(seeds[17], 3), SEQS // SEQ_DEV)
    routes = jax.vmap(lambda own, number: routed_block(jax.random.fold_in(seeds[17], 2), own, number, SEQ_DEV, EXPERTS, TOPK, CAP, 2))(routes_keys, routes_turns).reshape((SEQS, TOPK))
    route_gates = jnp.clip(jnp.exp(math.log(1.0) - 2.9957323 * jax.random.uniform(seeds[18], (SEQS, TOPK), jnp.float32) ** shard_levels(seeds[18], (SEQS, TOPK), ((0, 64),), -0.2, 0.2)), 0.05, 1.0)
    expert_gate = bell_draw(seeds[19], (EXPERTS, D, FF), (D // 9) ** -0.5, 0.375, ((0, 64), (2, 4)))
    expert_up = bell_draw(seeds[20], (EXPERTS, D, FF), (D // 9) ** -0.5, 0.375, ((0, 64), (2, 4)))
    expert_down = bell_draw(seeds[21], (EXPERTS, FF, D), FF ** -0.5, 0.125, ((0, 64), (1, 4)))
    out_gain = jnp.clip(1.0 + 0.18 * jax.random.normal(seeds[22], (D,), jnp.float32), 0.1, 1.9)
    return {"layer_in": layer_in, "state_in": state_in, "mix_gain": mix_gain, "rec_weight": rec_weight, "key_weight": key_weight, "val_weight": val_weight, "decay_down": decay_down, "decay_up": decay_up, "decay_base": decay_base, "rate_down": rate_down, "rate_up": rate_up, "rate_base": rate_base, "key_scale": key_scale, "group_gain": group_gain, "out_weight": out_weight, "post_gain": post_gain, "ffn_gain": ffn_gain, "routes": routes, "route_gates": route_gates, "expert_gate": expert_gate, "expert_up": expert_up, "expert_down": expert_down, "out_gain": out_gain}


norm_eps = 1e-06
group_eps = 0.00064
clamp_limit = 7.0
gate_alpha = 1.702

def rms_scale(values, scales):
    return values * lax.rsqrt(lax.optimization_barrier(jnp.mean(values * values, axis=-1, keepdims=True)) + norm_eps) * scales

def rounded(values):
    return lax.optimization_barrier(values.astype(jnp.bfloat16)).astype(jnp.float32)

def update_block(inputs):
    old_state, unit_key, decay_factor, learn_rate, val_rows, key_rows, rec_rows = inputs
    along_key = lax.optimization_barrier(jnp.sum(old_state * unit_key[:, :, None, :], axis=-1))
    new_state = old_state * decay_factor[:, :, None, :] - along_key[..., None] * (unit_key * learn_rate)[:, :, None, :] + val_rows[..., None] * (key_rows * learn_rate)[:, :, None, :]
    readout = lax.optimization_barrier(jnp.sum(new_state * rec_rows[:, :, None, :], axis=-1))
    return (new_state, readout)

def reference(layer_in, state_in, mix_gain, rec_weight, key_weight, val_weight, decay_down, decay_up, decay_base, rate_down, rate_up, rate_base, key_scale, group_gain, out_weight, post_gain, ffn_gain, routes, route_gates, expert_gate, expert_up, expert_down, out_gain):
    normed_in = rms_scale(layer_in.astype(jnp.float32), mix_gain).astype(jnp.bfloat16)
    rec_full = rounded(jnp.dot(normed_in, rec_weight, preferred_element_type=jnp.float32))
    key_full = rounded(jnp.dot(normed_in, key_weight, preferred_element_type=jnp.float32))
    val_full = rounded(jnp.dot(normed_in, val_weight, preferred_element_type=jnp.float32))
    decay_hidden = jnp.tanh(jnp.dot(normed_in, decay_down, preferred_element_type=jnp.float32)).astype(jnp.bfloat16)
    rate_hidden = jnp.dot(normed_in, rate_down, preferred_element_type=jnp.float32).astype(jnp.bfloat16)
    decay_pre = decay_base + jnp.dot(decay_hidden, decay_up, preferred_element_type=jnp.float32)
    decay_factor = jnp.exp(-jnp.exp(-jax.nn.softplus(-decay_pre) - 0.5))
    learn_rate = jax.nn.sigmoid(rate_base + jnp.dot(rate_hidden, rate_up, preferred_element_type=jnp.float32))
    head_shape = (N_EP, SEQ_DEV, HEADS, HEAD_DIM)
    key_heads = key_full.reshape(head_shape)
    scaled_key = key_heads * key_scale.reshape(HEADS, HEAD_DIM)
    unit_key = scaled_key * lax.rsqrt(lax.optimization_barrier(jnp.sum(scaled_key * scaled_key, axis=-1, keepdims=True)) + norm_eps)
    old_state = state_in.reshape(N_EP, SEQ_DEV, HEADS, HEAD_DIM, HEAD_DIM)
    new_state, readout = lax.map(update_block, (old_state, unit_key, decay_factor.reshape(head_shape), learn_rate.reshape(head_shape), val_full.reshape(head_shape), key_heads, rec_full.reshape(head_shape)))
    readout = readout.reshape(SEQS, HEADS, HEAD_DIM)
    centred = readout - lax.optimization_barrier(jnp.mean(readout, axis=-1, keepdims=True))
    normed_out = centred * lax.rsqrt(lax.optimization_barrier(jnp.mean(centred * centred, axis=-1, keepdims=True)) + group_eps)
    normed_out = (normed_out * group_gain.reshape(HEADS, HEAD_DIM)).reshape(SEQS, D).astype(jnp.bfloat16)
    grouped_out = normed_out.astype(jnp.float32).reshape(SEQS, N_TP, D // N_TP)
    grouped_weight = out_weight.astype(jnp.float32).reshape(N_TP, D // N_TP, D)
    partials = jnp.einsum('sgc,gcd->gsd', grouped_out, grouped_weight)
    mix_sum = lax.optimization_barrier(jnp.sum(rounded(partials), axis=0))
    middle = (layer_in.astype(jnp.float32) + rms_scale(mix_sum, post_gain)).astype(jnp.bfloat16)
    ffn_in = rms_scale(middle.astype(jnp.float32), ffn_gain).astype(jnp.bfloat16)
    flat_routes = routes.reshape(N_EP, SEQ_DEV * TOPK)
    onehot = (flat_routes[:, :, None] == jnp.arange(EXPERTS, dtype=jnp.int32)[None, None, :]).astype(jnp.int32)
    slot_rank = lax.optimization_barrier(jnp.sum((jnp.cumsum(onehot, axis=1) - 1) * onehot, axis=2))
    source = jnp.arange(N_EP, dtype=jnp.int32)[:, None]
    slot_index = (flat_routes * (N_EP * CAP) + source * CAP + slot_rank).reshape(-1).astype(jnp.int32)
    token_index = jnp.arange(SEQS * TOPK, dtype=jnp.int32) // TOPK
    slot_token = jnp.full((EXPERTS * N_EP * CAP,), SEQS, jnp.int32).at[slot_index].set(token_index)
    padded_in = jnp.concatenate([ffn_in, jnp.zeros((1, D), jnp.bfloat16)], axis=0)

    def run_expert(inputs):
        tokens, w_gate, w_up, w_down = inputs
        taken_rows = padded_in[tokens]
        gate_cut = jnp.minimum(jnp.dot(taken_rows, w_gate, preferred_element_type=jnp.float32), clamp_limit)
        up_cut = jnp.clip(jnp.dot(taken_rows, w_up, preferred_element_type=jnp.float32), -clamp_limit, clamp_limit)
        hidden = ((up_cut + 1.0) * gate_cut * jax.nn.sigmoid(gate_alpha * gate_cut)).astype(jnp.bfloat16)
        grouped = hidden.astype(jnp.float32).reshape(tokens.shape[0], N_TP, FF // N_TP)
        down_groups = w_down.astype(jnp.float32).reshape(N_TP, FF // N_TP, D)
        parts = jnp.einsum('rgf,gfd->grd', grouped, down_groups)
        return lax.optimization_barrier(jnp.sum(rounded(parts), axis=0)).astype(jnp.bfloat16)
    expert_rows = lax.map(run_expert, (slot_token.reshape(EXPERTS, N_EP * CAP), expert_gate, expert_up, expert_down))
    picked = expert_rows.reshape(-1, D)[slot_index].reshape(SEQS, TOPK, D)
    moe_sum = lax.optimization_barrier(jnp.sum(route_gates[:, :, None] * picked.astype(jnp.float32), axis=1))
    layer_out = (middle.astype(jnp.float32) + rms_scale(moe_sum, out_gain)).astype(jnp.bfloat16)
    return (layer_out, new_state.reshape(SEQS, HEADS, HEAD_DIM * HEAD_DIM))
```

```python
import functools

import jax
import jax.numpy as jnp
from jax import lax
from jax.experimental import pallas as pl
from jax.experimental.pallas import tpu as pltpu
from jax.sharding import PartitionSpec as P

MESH = pl.DeviceIdType.MESH
HEAD_DIM = 64
CAP = 2
LANES = 128
WIDE = 256

norm_eps = 1e-06
group_eps = 0.00064
clamp_limit = 7.0
gate_alpha = 1.702

F32 = jnp.float32
BF16 = jnp.bfloat16


def dot(a, b):
    return lax.dot_general(a, b, (((1,), (0,)), ((), ())), preferred_element_type=F32)


def dot_t(a, b):
    return lax.dot_general(a, b, (((1,), (1,)), ((), ())), preferred_element_type=F32)


def split(a):
    high = a.astype(BF16)
    return high, (a - high.astype(F32)).astype(BF16)


def dot_split(a, b):
    high, low = split(a)
    return dot(high, b) + dot(low, b)


def iota(shape, dim):
    return lax.broadcasted_iota(jnp.int32, shape, dim)


def one_hot(mask):
    return jnp.where(mask, 1.0, 0.0).astype(BF16)


def rms_scale(values, scales):
    return values * lax.rsqrt(jnp.mean(values * values, axis=-1, keepdims=True) + norm_eps) * scales


def kernel(
    n_ep,
    n_tp,
    layer_in,
    state_in,
    mix_gain,
    rec_weight,
    key_weight,
    val_weight,
    decay_down,
    decay_up,
    decay_base,
    rate_down,
    rate_up,
    rate_base,
    key_scale,
    group_gain,
    out_weight,
    post_gain,
    ffn_gain,
    routes_t,
    routes,
    gates,
    expert_gate,
    expert_up,
    expert_down,
    out_gain,
    layer_out,
    new_state,
    state,
    w_gate,
    w_up,
    w_down,
    proj_send,
    proj_all,
    out_send,
    out_all,
    rows_all,
    normed_all,
    qkv_send,
    qkv_all,
    decay_rows,
    rate_rows,
    read_send,
    read_all,
    part_send,
    part_all,
    mix_rows,
    wide_rows,
    slot_send,
    slot_here,
    slot_all,
    down_send,
    down_all,
    back_send,
    back_all,
    moe_send,
    moe_all,
    load_sem,
    send_sem,
    recv_sem,
    slot_sem,
):
    seqs, width = layer_in.shape
    heads = state_in.shape[1]
    plane = heads
    n_z = n_ep // plane
    low = decay_down.shape[1]
    quarter = width // n_tp
    tiles = quarter // LANES
    slab = CAP * tiles
    rows = seqs * heads
    depth = rec_weight.shape[0]
    out_cols = out_weight.shape[1]

    me = lax.axis_index("ep")
    mine = lax.axis_index("tp")
    member = lax.rem(me, plane)
    base = me - member

    def ep_at(step):
        return lax.rem(me + step, n_ep)

    def member_at(step):
        return lax.rem(member + step, plane)

    def z_at(step):
        return lax.rem(me + step * plane, n_ep)

    def tp_at(step):
        return lax.rem(mine + step, n_tp)

    def send(src, dst, phase, ep, tp, sem=None):
        pltpu.make_async_remote_copy(
            src_ref=src,
            dst_ref=dst,
            send_sem=send_sem.at[phase],
            recv_sem=recv_sem.at[phase] if sem is None else sem,
            device_id={"ep": ep, "tp": tp},
            device_id_type=MESH,
        ).start()

    def keep(src, dst, sem):
        pltpu.make_async_copy(src, dst, sem).start()

    def arrive(buffer, sem):
        pltpu.make_async_copy(buffer, buffer, sem).wait()

    def sent(buffer, phase):
        pltpu.make_async_copy(buffer, buffer, send_sem.at[phase]).wait()

    def loop(start, stop, body):
        def step(i, carry):
            body(i)
            return carry

        lax.fori_loop(start, stop, step, 0)

    barrier = pltpu.get_barrier_semaphore()

    def greet(i):
        pl.semaphore_signal(barrier, inc=1, device_id={"ep": ep_at(i), "tp": mine}, device_id_type=MESH)

    loop(1, n_ep, greet)

    def greet_plane(i):
        pl.semaphore_signal(
            barrier,
            inc=1,
            device_id={"ep": base + member_at(lax.rem(i, plane)), "tp": tp_at(i // plane)},
            device_id_type=MESH,
        )

    loop(plane, plane * n_tp, greet_plane)

    loads = (
        (state_in, state),
        (expert_gate.at[0], w_gate),
        (expert_up.at[0], w_up),
        (expert_down.at[0], w_down),
    )
    for n, (src, dst) in enumerate(loads):
        pltpu.make_async_copy(src, dst, load_sem.at[n]).start()

    for h in range(heads):
        cut = slice(h * HEAD_DIM, (h + 1) * HEAD_DIM)
        proj_send[h, :depth, :] = jnp.concatenate([rec_weight[:, cut], key_weight[:, cut]], axis=1)
        proj_send[h, depth:, :] = jnp.concatenate(
            [val_weight[: depth // 2, cut], val_weight[depth // 2 :, cut]], axis=1
        )
    eye = one_hot(iota((out_cols, out_cols), 0) == iota((out_cols, out_cols), 1))
    out_send[...] = dot_t(eye, out_weight[...]).astype(BF16)

    pl.semaphore_wait(barrier, n_ep - 1 + plane * (n_tp - 1))

    keep(layer_in, rows_all.at[member], recv_sem.at[0])

    def send_rows(i):
        send(layer_in, rows_all.at[member], 0, base + member_at(i), mine)

    loop(1, plane, send_rows)
    keep(proj_send.at[member], proj_all.at[me], recv_sem.at[1])

    def send_proj(i):
        to = ep_at(i)
        send(proj_send.at[lax.rem(to, plane)], proj_all.at[me], 1, to, mine)

    loop(1, n_ep, send_proj)
    z_me = me // plane
    keep(out_send, out_all.at[z_me], recv_sem.at[2])

    def send_out(i):
        send(out_send, out_all.at[z_me], 2, z_at(i), mine)

    loop(1, n_z, send_out)

    own_normed = rms_scale(layer_in[...].astype(F32), mix_gain[...]).astype(BF16)
    decay_hidden = jnp.tanh(dot(own_normed, decay_down[...])).astype(BF16)
    rate_hidden = dot(own_normed, rate_down[...]).astype(BF16)
    decay_sig = jax.nn.sigmoid(decay_base[...] + dot(decay_hidden, decay_up[...]))
    decay = jnp.exp(-jnp.exp(jnp.full((), -0.5, F32)) * decay_sig)
    rate = jax.nn.sigmoid(rate_base[...] + dot(rate_hidden, rate_up[...]))
    for h in range(heads):
        cut = slice(h * HEAD_DIM, (h + 1) * HEAD_DIM)
        decay_rows[h * seqs : (h + 1) * seqs, :] = decay[:, cut]
        rate_rows[h * seqs : (h + 1) * seqs, :] = rate[:, cut]

    top = routes.shape[1]
    named_t = jnp.zeros((n_ep, seqs), F32)
    for j in range(top):
        named_t += jnp.where(iota((n_ep, seqs), 0) == routes_t[j : j + 1, :], 1.0, 0.0)
    before_t = dot(named_t.astype(BF16), one_hot(iota((seqs, seqs), 0) < iota((seqs, seqs), 1)))
    named = jnp.zeros((seqs, n_ep), F32)
    weight = jnp.zeros((seqs, n_ep), F32)
    for j in range(top):
        hit = iota((seqs, n_ep), 1) == routes[:, j : j + 1]
        named += jnp.where(hit, 1.0, 0.0)
        weight += jnp.where(hit, gates[:, j : j + 1], 0.0)
    before = dot(one_hot(iota((seqs, seqs), 1) < iota((seqs, seqs), 0)), named.astype(BF16))

    arrive(rows_all, recv_sem.at[0])

    def norm_rows(i):
        values = rms_scale(rows_all[i].astype(F32), mix_gain[...]).astype(BF16)
        normed_all[pl.ds(pl.multiple_of(i * seqs, seqs), seqs), :] = values

    loop(0, plane, norm_rows)

    arrive(proj_all, recv_sem.at[1])
    pairs = proj_all[:, :depth, :].reshape(n_ep * depth, 2 * HEAD_DIM)
    vals = proj_all[:, depth:, :]
    vals = jnp.concatenate([vals, vals], axis=1).reshape(n_ep * depth, 2 * HEAD_DIM)
    spread = (n_ep * depth, 2 * HEAD_DIM)
    first = lax.rem(iota(spread, 0), depth) < depth // 2
    vals = jnp.where(first == (iota(spread, 1) < HEAD_DIM), vals.astype(F32), 0.0).astype(BF16)
    normed = normed_all[...]
    pair_sum = dot(normed, pairs)
    val_sum = dot(normed, vals)
    val_sum = val_sum[:, :HEAD_DIM] + val_sum[:, HEAD_DIM:]
    together = jnp.concatenate([pair_sum, val_sum, jnp.zeros_like(val_sum)], axis=1)
    qkv_send[...] = together.astype(BF16).reshape(plane, seqs, WIDE)
    keep(qkv_send.at[member], qkv_all.at[member], recv_sem.at[3])

    def send_qkv(i):
        to = member_at(i)
        send(qkv_send.at[to], qkv_all.at[member], 3, base + to, mine)

    loop(1, plane, send_qkv)

    turn = one_hot(
        iota((rows, rows), 1)
        == lax.rem(iota((rows, rows), 0), heads) * seqs + iota((rows, rows), 0) // heads
    )
    turn_back = one_hot(
        iota((rows, rows), 1)
        == lax.rem(iota((rows, rows), 0), seqs) * heads + iota((rows, rows), 0) // seqs
    )
    decay_high, decay_low = split(decay_rows[...])
    rate_high, rate_low = split(rate_rows[...])
    turned = dot(turn, jnp.concatenate([decay_high, decay_low, rate_high, rate_low], axis=1))
    decay = turned[:, :HEAD_DIM] + turned[:, HEAD_DIM : 2 * HEAD_DIM]
    rate = turned[:, 2 * HEAD_DIM : 3 * HEAD_DIM] + turned[:, 3 * HEAD_DIM :]
    joined = one_hot(iota((WIDE, WIDE), 0) // HEAD_DIM == iota((WIDE, WIDE), 1) // HEAD_DIM)

    arrive(qkv_all, recv_sem.at[3])
    qkv = dot(turn, qkv_all[...].reshape(rows, WIDE))
    rec = qkv[:, :HEAD_DIM]
    key = qkv[:, HEAD_DIM : 2 * HEAD_DIM]
    val = qkv[:, 2 * HEAD_DIM : 3 * HEAD_DIM].astype(BF16)

    def of_heads(scales):
        return jnp.broadcast_to(scales[...][None], (seqs, heads, HEAD_DIM)).reshape(rows, HEAD_DIM)

    scaled = key * of_heads(key_scale)
    unit = scaled * lax.rsqrt(jnp.sum(scaled * scaled, axis=-1, keepdims=True) + norm_eps)

    def wide(a):
        return jnp.concatenate([a] * (WIDE // HEAD_DIM), axis=1)

    unit_w, decay_w, rec_w = wide(unit), wide(decay), wide(rec)
    unit_rate, key_rate = wide(unit * rate), wide(key * rate)
    per = WIDE // HEAD_DIM
    pltpu.make_async_copy(state_in, state, load_sem.at[0]).wait()

    def update(i, readout):
        lanes = pl.ds(pl.multiple_of(i * WIDE, WIDE), WIDE)
        old = state[:, :, lanes].reshape(rows, WIDE)
        along = dot_split(old * unit_w, joined)
        pick = one_hot(iota((HEAD_DIM, WIDE), 0) == i * per + iota((HEAD_DIM, WIDE), 1) // HEAD_DIM)
        gather = one_hot(iota((WIDE, HEAD_DIM), 1) == i * per + iota((WIDE, HEAD_DIM), 0) // HEAD_DIM)
        new = old * decay_w - along * unit_rate + dot(val, pick) * key_rate
        state[:, :, lanes] = new.reshape(seqs, heads, WIDE)
        return readout + dot_split(new * rec_w, gather)

    readout = lax.fori_loop(0, HEAD_DIM // per, update, jnp.zeros((rows, HEAD_DIM), F32))
    centred = readout - jnp.mean(readout, axis=-1, keepdims=True)
    normed_out = centred * lax.rsqrt(jnp.mean(centred * centred, axis=-1, keepdims=True) + group_eps)
    normed_out = dot(turn_back, (normed_out * of_heads(group_gain)).astype(BF16)).astype(BF16)
    for h in range(heads):
        read_send[:, h * HEAD_DIM : (h + 1) * HEAD_DIM] = normed_out[h * seqs : (h + 1) * seqs, :]
    keep(read_send, read_all.at[member], recv_sem.at[4])

    def send_read(i):
        send(read_send, read_all.at[member], 4, base + member_at(i), mine)

    loop(1, plane, send_read)
    pltpu.make_async_copy(state, new_state, load_sem.at[0]).start()

    arrive(out_all, recv_sem.at[2])
    arrive(read_all, recv_sem.at[4])
    part = dot_t(
        read_all[...].reshape(plane * seqs, quarter), out_all[...].reshape(n_z * out_cols, quarter)
    )
    part_send[...] = part.astype(BF16).reshape(plane, seqs, n_z * out_cols)
    keep(part_send.at[member], part_all.at[mine * plane + member], recv_sem.at[5])

    def send_part(i):
        to = member_at(lax.rem(i, plane))
        send(part_send.at[to], part_all.at[mine * plane + member], 5, base + to, tp_at(i // plane))

    loop(1, plane * n_tp, send_part)

    arrive(part_all, recv_sem.at[5])
    for g in range(plane):
        total = part_all[g].astype(F32)
        for t in range(1, n_tp):
            total += part_all[t * plane + g].astype(F32)
        for z in range(n_z):
            at = (z * plane + g) * out_cols
            mix_rows[:, at : at + out_cols] = total[:, z * out_cols : (z + 1) * out_cols]
    middle = (layer_in[...].astype(F32) + rms_scale(mix_rows[...], post_gain[...])).astype(BF16)
    mix_rows[...] = middle.astype(F32)
    ffn_in = rms_scale(mix_rows[...], ffn_gain[...])

    mix_rows[...] = ffn_in
    columns = pl.ds(pl.multiple_of(mine * quarter, quarter), quarter)
    ffn_cut = mix_rows[:, columns].astype(BF16)
    for s in range(CAP):
        chosen = jnp.where(before_t == float(s), named_t, 0.0).astype(BF16)
        values = dot(chosen, ffn_cut)
        for t in range(tiles):
            wide_rows[pl.ds(s * tiles + t, n_ep, stride=slab), :] = values[:, t * LANES : (t + 1) * LANES]
    slot_send[...] = wide_rows[...].astype(BF16).reshape(n_ep, slab, LANES)
    keep(slot_send.at[me], slot_here.at[me], recv_sem.at[6])

    def send_slot(i):
        to = ep_at(i)
        send(slot_send.at[to], slot_here.at[me], 6, to, mine)

    loop(1, n_ep, send_slot)
    mix_rows[...] = middle.astype(F32)

    arrive(slot_here, recv_sem.at[6])
    for step in range(1, n_tp):
        send(slot_here, slot_all.at[mine], 7, me, tp_at(step), slot_sem.at[mine])

    pltpu.make_async_copy(expert_gate.at[0], w_gate, load_sem.at[1]).wait()
    pltpu.make_async_copy(expert_up.at[0], w_up, load_sem.at[2]).wait()
    slots = CAP * n_ep

    def from_slabs(source):
        wide_rows[...] = source.astype(F32).reshape(n_ep * slab, LANES)
        return [
            [wide_rows[pl.ds(s * tiles + t, n_ep, stride=slab), :] for t in range(tiles)]
            for s in range(CAP)
        ]

    gate = up = None
    order = [0, 1, n_tp - 1] + list(range(2, n_tp - 1))
    for step in order[:n_tp]:
        at = tp_at(step)
        if step == 0:
            source = slot_here[...]
        else:
            arrive(slot_all.at[at], slot_sem.at[at])
            source = slot_all[at]
        part = jnp.concatenate([jnp.concatenate(p, axis=1) for p in from_slabs(source)], axis=0).astype(BF16)
        feats = pl.ds(pl.multiple_of(at * quarter, quarter), quarter)
        gate_part, up_part = dot(part, w_gate[feats, :]), dot(part, w_up[feats, :])
        gate = gate_part if gate is None else gate + gate_part
        up = up_part if up is None else up + up_part
    gate = jnp.minimum(gate, clamp_limit)
    up = jnp.clip(up, -clamp_limit, clamp_limit)
    hidden = ((up + 1.0) * gate * jax.nn.sigmoid(gate_alpha * gate)).astype(BF16)

    pltpu.make_async_copy(expert_down.at[0], w_down, load_sem.at[3]).wait()
    for step in list(range(1, n_tp)) + [0]:
        at = tp_at(step)
        feats = pl.ds(pl.multiple_of(at * quarter, quarter), quarter)
        values = dot(hidden, w_down[:, feats]).astype(BF16)
        if step == 0:
            down_all[mine] = values
        else:
            down_send[at] = values
            send(down_send.at[at], down_all.at[mine], 8, me, at, slot_sem.at[n_tp + mine])
    for step in range(1, n_tp):
        at = tp_at(step)
        arrive(down_all.at[at], slot_sem.at[n_tp + at])
    total = down_all[0].astype(F32)
    for t in range(1, n_tp):
        total += down_all[t].astype(F32)
    for s in range(CAP):
        for t in range(tiles):
            wide_rows[pl.ds(s * tiles + t, n_ep, stride=slab), :] = total[
                s * n_ep : (s + 1) * n_ep, t * LANES : (t + 1) * LANES
            ]
    back_send[...] = wide_rows[...].astype(BF16).reshape(n_ep, slab, LANES)
    keep(back_send.at[me], back_all.at[me], recv_sem.at[9])

    def send_back(i):
        to = ep_at(i)
        send(back_send.at[to], back_all.at[me], 9, to, mine)

    loop(1, n_ep, send_back)

    arrive(back_all, recv_sem.at[9])
    moe = jnp.zeros((seqs, quarter), F32)
    for s, p in enumerate(from_slabs(back_all[...])):
        moe += dot_split(jnp.where(before == float(s), weight, 0.0), jnp.concatenate(p, axis=1).astype(BF16))
    moe_send[...] = moe
    keep(moe_send, moe_all.at[mine], recv_sem.at[10])
    for step in range(1, n_tp):
        send(moe_send, moe_all.at[mine], 10, me, tp_at(step))
    arrive(moe_all, recv_sem.at[10])
    moe = jnp.concatenate([moe_all[t] for t in range(n_tp)], axis=1)
    layer_out[...] = (mix_rows[...] + rms_scale(moe, out_gain[...])).astype(BF16)

    pltpu.make_async_copy(state, new_state, load_sem.at[0]).wait()
    sent(rows_all.at[pl.ds(0, plane - 1)], 0)
    sent(proj_all.at[pl.ds(0, n_ep - 1)], 1)
    sent(out_all.at[pl.ds(0, n_z - 1)], 2)
    sent(qkv_all.at[pl.ds(0, plane - 1)], 3)
    sent(read_all.at[pl.ds(0, plane - 1)], 4)
    sent(part_all.at[pl.ds(0, n_tp * plane - 1)], 5)
    sent(slot_here.at[pl.ds(0, n_ep - 1)], 6)
    sent(slot_all.at[pl.ds(0, n_tp - 1)], 7)
    sent(down_all.at[pl.ds(0, n_tp - 1)], 8)
    sent(back_all.at[pl.ds(0, n_ep - 1)], 9)
    sent(moe_all.at[pl.ds(0, n_tp - 1)], 10)


def local(n_ep, n_tp, *args):
    (
        layer_in,
        state_in,
        mix_gain,
        rec_weight,
        key_weight,
        val_weight,
        decay_down,
        decay_up,
        decay_base,
        rate_down,
        rate_up,
        rate_base,
        key_scale,
        group_gain,
        out_weight,
        post_gain,
        ffn_gain,
        routes,
        route_gates,
        expert_gate,
        expert_up,
        expert_down,
        out_gain,
    ) = args
    seqs, width = layer_in.shape
    heads = state_in.shape[1]
    plane = heads
    n_z = n_ep // plane
    quarter = width // n_tp
    slab = CAP * (quarter // LANES)
    depth = rec_weight.shape[0]
    out_cols = out_weight.shape[1]
    hidden = expert_gate.shape[2]
    slots = CAP * n_ep
    state_lanes = state_in.shape[2]
    row = lambda a: a.reshape(1, -1)
    by_head = lambda a: a.reshape(heads, HEAD_DIM)
    operands = (
        layer_in,
        state_in,
        row(mix_gain),
        rec_weight,
        key_weight,
        val_weight,
        decay_down,
        decay_up,
        row(decay_base),
        rate_down,
        rate_up,
        row(rate_base),
        by_head(key_scale),
        by_head(group_gain),
        out_weight,
        row(post_gain),
        row(ffn_gain),
        routes.T,
        routes,
        route_gates,
        expert_gate,
        expert_up,
        expert_down,
        row(out_gain),
    )
    far = {1, 20, 21, 22}
    vmem = pl.BlockSpec(memory_space=pltpu.VMEM)
    hbm = pl.BlockSpec(memory_space=pl.ANY)
    scratch = [
        pltpu.VMEM(state_in.shape, F32),
        pltpu.VMEM((width, hidden), BF16),
        pltpu.VMEM((width, hidden), BF16),
        pltpu.VMEM((hidden, width), BF16),
        pltpu.VMEM((plane, depth + depth // 2, 2 * HEAD_DIM), BF16),
        pltpu.VMEM((n_ep, depth + depth // 2, 2 * HEAD_DIM), BF16),
        pltpu.VMEM((out_cols, quarter), BF16),
        pltpu.VMEM((n_z, out_cols, quarter), BF16),
        pltpu.VMEM((plane, seqs, width), BF16),
        pltpu.VMEM((plane * seqs, width), BF16),
        pltpu.VMEM((plane, seqs, WIDE), BF16),
        pltpu.VMEM((plane, seqs, WIDE), BF16),
        pltpu.VMEM((heads * seqs, HEAD_DIM), F32),
        pltpu.VMEM((heads * seqs, HEAD_DIM), F32),
        pltpu.VMEM((seqs, quarter), BF16),
        pltpu.VMEM((plane, seqs, quarter), BF16),
        pltpu.VMEM((plane, seqs, n_z * out_cols), BF16),
        pltpu.VMEM((n_tp * plane, seqs, n_z * out_cols), BF16),
        pltpu.VMEM((seqs, width), F32),
        pltpu.VMEM((n_ep * slab, LANES), F32),
        pltpu.VMEM((n_ep, slab, LANES), BF16),
        pltpu.VMEM((n_ep, slab, LANES), BF16),
        pltpu.VMEM((n_tp, n_ep, slab, LANES), BF16),
        pltpu.VMEM((n_tp, slots, quarter), BF16),
        pltpu.VMEM((n_tp, slots, quarter), BF16),
        pltpu.VMEM((n_ep, slab, LANES), BF16),
        pltpu.VMEM((n_ep, slab, LANES), BF16),
        pltpu.VMEM((seqs, quarter), F32),
        pltpu.VMEM((n_tp, seqs, quarter), F32),
        pltpu.SemaphoreType.DMA((4,)),
        pltpu.SemaphoreType.DMA((11,)),
        pltpu.SemaphoreType.DMA((11,)),
        pltpu.SemaphoreType.DMA((2 * n_tp,)),
    ]
    return pl.pallas_call(
        functools.partial(kernel, n_ep, n_tp),
        out_shape=(
            jax.ShapeDtypeStruct(layer_in.shape, BF16),
            jax.ShapeDtypeStruct((seqs, heads, state_lanes), F32),
        ),
        in_specs=[hbm if n in far else vmem for n in range(len(operands))],
        out_specs=(vmem, hbm),
        scratch_shapes=scratch,
        compiler_params=pltpu.CompilerParams(
            collective_id=0, has_side_effects=True, vmem_limit_bytes=48 * 1024 * 1024
        ),
    )(*operands)


def solution(mesh):
    in_specs = (
        P("ep", None),
        P("ep", "tp", None),
        P(),
        P("ep", "tp"),
        P("ep", "tp"),
        P("ep", "tp"),
        P(),
        P(None, "tp"),
        P("tp"),
        P(),
        P(None, "tp"),
        P("tp"),
        P("tp"),
        P("tp"),
        P("tp", "ep"),
        P(),
        P(),
        P("ep", None),
        P("ep", None),
        P("ep", None, "tp"),
        P("ep", None, "tp"),
        P("ep", "tp", None),
        P(),
    )
    out_specs = (P("ep", None), P("ep", "tp", None))
    body = functools.partial(local, mesh.shape["ep"], mesh.shape["tp"])
    return jax.shard_map(body, mesh=mesh, in_specs=in_specs, out_specs=out_specs, check_vma=False)
```

```python
import functools

import jax
import jax.numpy as jnp
from jax import lax
from jax.experimental import pallas as pl
from jax.experimental.pallas import tpu as pltpu
from jax.sharding import PartitionSpec as P

MESH = pl.DeviceIdType.MESH
HEAD_DIM = 64
CAP = 2
LANES = 128
WIDE = 256

norm_eps = 1e-06
group_eps = 0.00064
clamp_limit = 7.0
gate_alpha = 1.702

F32 = jnp.float32
BF16 = jnp.bfloat16


def dot(a, b):
    return lax.dot_general(a, b, (((1,), (0,)), ((), ())), preferred_element_type=F32)


def dot_t(a, b):
    return lax.dot_general(a, b, (((1,), (1,)), ((), ())), preferred_element_type=F32)


def split(a):
    high = a.astype(BF16)
    return high, (a - high.astype(F32)).astype(BF16)


def dot_split(a, b):
    high, low = split(a)
    return dot(high, b) + dot(low, b)


def iota(shape, dim):
    return lax.broadcasted_iota(jnp.int32, shape, dim)


def one_hot(mask):
    return jnp.where(mask, 1.0, 0.0).astype(BF16)


def rms_scale(values, scales):
    return values * lax.rsqrt(jnp.mean(values * values, axis=-1, keepdims=True) + norm_eps) * scales


def kernel(
    n_ep,
    n_tp,
    layer_in_far,
    rec_weight_far,
    key_weight_far,
    val_weight_far,
    out_weight_t_far,
    mix_gain_far,
    decay_down_t_far,
    rate_down_t_far,
    decay_up_far,
    rate_up_far,
    decay_base_far,
    rate_base_far,
    key_scale_far,
    group_gain_far,
    routes_t_far,
    gates_t_far,
    post_gain_far,
    ffn_gain_far,
    out_gain_far,
    state_far,
    expert_gate_far,
    expert_up_far,
    expert_down_far,
    layer_out,
    new_state,
    layer_in,
    rec_weight,
    key_weight,
    val_weight,
    out_send,
    mix_gain,
    decay_down_t,
    rate_down_t,
    decay_up,
    rate_up,
    decay_base,
    rate_base,
    key_scale,
    group_gain,
    routes_t,
    gates_t,
    post_gain,
    ffn_gain,
    out_gain,
    state,
    w_gate,
    w_up,
    w_down,
    proj_send,
    proj_all,
    out_all,
    rows_all,
    normed_all,
    qkv_send,
    qkv_all,
    decay_rows,
    rate_rows,
    by_head,
    gather_all,
    pick_all,
    read_send,
    read_all,
    part_send,
    part_all,
    mix_rows,
    wide_rows,
    slot_send,
    slot_here,
    slot_far_send,
    slot_far,
    slot_all,
    down_send,
    down_all,
    back_send,
    back_all,
    back_far_send,
    back_far,
    moe_send,
    moe_all,
    load_sem,
    send_sem,
    recv_sem,
    proj_sem,
    slot_sem,
):
    far = (
        layer_in_far,
        rec_weight_far,
        key_weight_far,
        val_weight_far,
        out_weight_t_far,
        mix_gain_far,
        decay_down_t_far,
        rate_down_t_far,
        decay_up_far,
        rate_up_far,
        decay_base_far,
        rate_base_far,
        key_scale_far,
        group_gain_far,
        routes_t_far,
        gates_t_far,
        post_gain_far,
        ffn_gain_far,
        out_gain_far,
        state_far,
        expert_gate_far.at[0],
        expert_up_far.at[0],
        expert_down_far.at[0],
    )
    near = (
        layer_in,
        rec_weight,
        key_weight,
        val_weight,
        out_send,
        mix_gain,
        decay_down_t,
        rate_down_t,
        decay_up,
        rate_up,
        decay_base,
        rate_base,
        key_scale,
        group_gain,
        routes_t,
        gates_t,
        post_gain,
        ffn_gain,
        out_gain,
        state,
        w_gate,
        w_up,
        w_down,
    )
    loads = [pltpu.make_async_copy(a, b, load_sem.at[n]) for n, (a, b) in enumerate(zip(far, near))]
    first_big = len(loads) - 4
    seqs, width = layer_in.shape
    heads = state.shape[1]
    plane = heads
    n_z = n_ep // plane
    quarter = width // n_tp
    tiles = quarter // LANES
    slab = CAP * tiles
    rows = seqs * heads
    depth = rec_weight.shape[0]
    out_cols = out_send.shape[0]

    for load in loads[:first_big]:
        load.start()

    me = lax.axis_index("ep")
    mine = lax.axis_index("tp")
    member = lax.rem(me, plane)
    base = me - member

    def member_at(step):
        return lax.rem(member + step, plane)

    def z_at(step):
        return lax.rem(me + step * plane, n_ep)

    def tp_at(step):
        return lax.rem(mine + step, n_tp)

    def send(src, dst, phase, ep, tp, sem=None):
        pltpu.make_async_remote_copy(
            src_ref=src,
            dst_ref=dst,
            send_sem=send_sem.at[phase],
            recv_sem=recv_sem.at[phase] if sem is None else sem,
            device_id={"ep": ep, "tp": tp},
            device_id_type=MESH,
        ).start()

    def keep(src, dst, sem):
        pltpu.make_async_copy(src, dst, sem).start()

    def arrive(buffer, sem):
        pltpu.make_async_copy(buffer, buffer, sem).wait()

    def sent(buffer, phase):
        pltpu.make_async_copy(buffer, buffer, send_sem.at[phase]).wait()

    def loop(start, stop, body):
        def step(i, carry):
            body(i)
            return carry

        lax.fori_loop(start, stop, step, 0)

    barrier = pltpu.get_barrier_semaphore()

    def others(body):
        for k in range(n_z):
            away = n_z // 2 + (k + 1) // 2 * (1 if k % 2 else -1)
            first = lax.rem(base + away % n_z * plane, n_ep)
            loop(0 if away % n_z else 1, plane, lambda i, first=first: body(first + member_at(i)))

    def greet(to):
        pl.semaphore_signal(barrier, inc=1, device_id={"ep": to, "tp": mine}, device_id_type=MESH)

    others(greet)

    def greet_plane(i):
        pl.semaphore_signal(
            barrier,
            inc=1,
            device_id={"ep": base + member_at(lax.rem(i, plane)), "tp": tp_at(i // plane)},
            device_id_type=MESH,
        )

    loop(plane, plane * n_tp, greet_plane)

    for load in loads[:5]:
        load.wait()
    for h in range(heads):
        cut = slice(h * HEAD_DIM, (h + 1) * HEAD_DIM)
        proj_send[h, :depth, :] = jnp.concatenate([rec_weight[:, cut], key_weight[:, cut]], axis=1)
        proj_send[h, depth:, :] = jnp.concatenate(
            [val_weight[: depth // 2, cut], val_weight[depth // 2 :, cut]], axis=1
        )
    for load in loads[first_big:]:
        load.start()
    for load in loads[5:first_big]:
        load.wait()
    pl.semaphore_wait(barrier, n_ep - 1 + plane * (n_tp - 1))

    keep(proj_send.at[member], proj_all.at[me], proj_sem.at[0])

    def send_proj(i, away):
        to = member_at(i)
        at = lax.rem(base + (n_z + away) * plane, n_ep) + to
        send(proj_send.at[to], proj_all.at[me], 1, at, mine, proj_sem.at[(n_z - away) % n_z])

    for away in (2, -2):
        loop(0, plane, functools.partial(send_proj, away=away))
    chip, core = member // 2, lax.rem(member, 2)
    keep(layer_in, rows_all.at[chip, core], recv_sem.at[0])

    def send_rows(i):
        send(layer_in, rows_all.at[chip, core], 0, base + member_at(2 * i), mine)

    loop(1, plane // 2, send_rows)
    for away in (1, -1):
        loop(0, plane, functools.partial(send_proj, away=away))
    loop(1, plane, functools.partial(send_proj, away=0))
    z_me = me // plane

    own_normed = rms_scale(layer_in[...].astype(F32), mix_gain[...]).astype(BF16)
    decay_hidden = jnp.tanh(dot_t(own_normed, decay_down_t[...])).astype(BF16)
    rate_hidden = dot_t(own_normed, rate_down_t[...]).astype(BF16)
    decay_sig = jax.nn.sigmoid(decay_base[...] + dot(decay_hidden, decay_up[...]))
    decay = jnp.exp(-jnp.exp(jnp.full((), -0.5, F32)) * decay_sig)
    rate = jax.nn.sigmoid(rate_base[...] + dot(rate_hidden, rate_up[...]))
    for h in range(heads):
        cut = slice(h * HEAD_DIM, (h + 1) * HEAD_DIM)
        decay_rows[h * seqs : (h + 1) * seqs, :] = decay[:, cut]
        rate_rows[h * seqs : (h + 1) * seqs, :] = rate[:, cut]
        by_head[0, h : h + 1, :] = key_scale[:, cut]
        by_head[1, h : h + 1, :] = group_gain[:, cut]

    top = routes_t.shape[0]
    named_t = jnp.zeros((n_ep, seqs), F32)
    weight_t = jnp.zeros((n_ep, seqs), F32)
    for j in range(top):
        hit = iota((n_ep, seqs), 0) == routes_t[j : j + 1, :]
        named_t += jnp.where(hit, 1.0, 0.0)
        weight_t += jnp.where(hit, gates_t[j : j + 1, :], 0.0)
    before_t = dot(named_t.astype(BF16), one_hot(iota((seqs, seqs), 0) < iota((seqs, seqs), 1)))
    eye = one_hot(iota((seqs, seqs), 0) == iota((seqs, seqs), 1))
    combine = []
    for s in range(CAP):
        high, low = split(jnp.where(before_t == float(s), weight_t, 0.0))
        combine.append((dot_t(eye, high).astype(BF16), dot_t(eye, low).astype(BF16)))
    per = WIDE // HEAD_DIM

    def tables(i):
        block = pl.ds(pl.multiple_of(i * WIDE, WIDE), WIDE)
        pick_all[:, block] = one_hot(
            iota((HEAD_DIM, WIDE), 0) == i * per + iota((HEAD_DIM, WIDE), 1) // HEAD_DIM
        )
        gather_all[block, :] = one_hot(
            iota((WIDE, HEAD_DIM), 1) == i * per + iota((WIDE, HEAD_DIM), 0) // HEAD_DIM
        )

    loop(0, HEAD_DIM // per, tables)

    def plane_of(away):
        at = lax.rem(base + (n_z + away) * plane, n_ep)
        return at, proj_all.at[pl.ds(at, plane)]

    half = plane // 2
    for away in (-2, 2):
        at, blocks = plane_of(away)
        arrive(blocks, proj_sem.at[away % n_z])
        side = -away // 2
        to = lax.rem(base + (n_z + side) * plane, n_ep) + member
        send(blocks, blocks, 1, to, mine, proj_sem.at[(away - side) % n_z])
        part = proj_all.at[pl.ds(at + (0 if side > 0 else half), half)]
        to = lax.rem(base + (n_z + 2 * side) * plane, n_ep) + member
        send(part, part, 1, to, mine, proj_sem.at[(away - 2 * side) % n_z])
    arrive(rows_all.at[:, core], recv_sem.at[0])
    sibling = me + 1 - 2 * core
    send(rows_all.at[:, core], rows_all.at[:, core], 13, sibling, mine)
    keep(out_send, out_all.at[z_me], recv_sem.at[2])

    def send_out(i):
        send(out_send, out_all.at[z_me], 2, z_at(i), mine)

    loop(1, n_z, send_out)

    arrive(rows_all.at[:, 1 - core], recv_sem.at[13])

    def norm_rows(i):
        values = rms_scale(rows_all[i // 2, lax.rem(i, 2)].astype(F32), mix_gain[...]).astype(BF16)
        normed_all[pl.ds(pl.multiple_of(i * seqs, seqs), seqs), :] = values

    loop(0, plane, norm_rows)

    for away in (0, 1, -1, 3, -3, 4):
        arrive(plane_of(away)[1], proj_sem.at[away % n_z])
    pairs = proj_all[:, :depth, :].reshape(n_ep * depth, 2 * HEAD_DIM)
    vals = proj_all[:, depth:, :]
    vals = jnp.concatenate([vals, vals], axis=1).reshape(n_ep * depth, 2 * HEAD_DIM)
    spread = (n_ep * depth, 2 * HEAD_DIM)
    first = lax.rem(iota(spread, 0), depth) < depth // 2
    vals = jnp.where(first == (iota(spread, 1) < HEAD_DIM), vals.astype(F32), 0.0).astype(BF16)
    normed = normed_all[...]
    pair_sum = dot(normed, pairs)
    val_sum = dot(normed, vals)
    val_sum = val_sum[:, :HEAD_DIM] + val_sum[:, HEAD_DIM:]
    together = jnp.concatenate([pair_sum, val_sum, jnp.zeros_like(val_sum)], axis=1)
    qkv_send[...] = together.astype(BF16).reshape(plane, seqs, WIDE)
    keep(qkv_send.at[member], qkv_all.at[member], recv_sem.at[3])

    def send_qkv(i):
        to = member_at(i)
        send(qkv_send.at[to], qkv_all.at[member], 3, base + to, mine)

    loop(1, plane, send_qkv)

    turn = one_hot(
        iota((rows, rows), 1)
        == lax.rem(iota((rows, rows), 0), heads) * seqs + iota((rows, rows), 0) // heads
    )
    turn_back = one_hot(
        iota((rows, rows), 1)
        == lax.rem(iota((rows, rows), 0), seqs) * heads + iota((rows, rows), 0) // seqs
    )
    decay_high, decay_low = split(decay_rows[...])
    rate_high, rate_low = split(rate_rows[...])
    turned = dot(turn, jnp.concatenate([decay_high, decay_low, rate_high, rate_low], axis=1))
    decay = turned[:, :HEAD_DIM] + turned[:, HEAD_DIM : 2 * HEAD_DIM]
    rate = turned[:, 2 * HEAD_DIM : 3 * HEAD_DIM] + turned[:, 3 * HEAD_DIM :]

    arrive(qkv_all, recv_sem.at[3])
    qkv = dot(turn, qkv_all[...].reshape(rows, WIDE))
    rec = qkv[:, :HEAD_DIM]
    key = qkv[:, HEAD_DIM : 2 * HEAD_DIM]
    val = qkv[:, 2 * HEAD_DIM : 3 * HEAD_DIM].astype(BF16)

    def of_heads(n):
        return jnp.broadcast_to(by_head[n][None], (seqs, heads, HEAD_DIM)).reshape(rows, HEAD_DIM)

    scaled = key * of_heads(0)
    unit = scaled * lax.rsqrt(jnp.sum(scaled * scaled, axis=-1, keepdims=True) + norm_eps)

    def wide(a):
        return jnp.concatenate([a] * (WIDE // HEAD_DIM), axis=1)

    unit_w, read_w = wide(unit), wide(decay * rec)
    loads[first_big].wait()

    def sums(i, totals):
        for k in range(4):
            block = pl.ds(pl.multiple_of((i * 4 + k) * WIDE, WIDE), WIDE)
            old = state[:, :, block].reshape(rows, WIDE)
            stacked = jnp.concatenate(split(old * unit_w) + split(old * read_w), axis=0)
            totals += dot(stacked, gather_all[block, :])
        return totals

    totals = lax.fori_loop(0, HEAD_DIM // per // 4, sums, jnp.zeros((4 * rows, HEAD_DIM), F32))
    along = totals[:rows] + totals[rows : 2 * rows]
    along_read = jnp.sum(unit * rate * rec, axis=-1, keepdims=True)
    val_read = jnp.sum(key * rate * rec, axis=-1, keepdims=True)
    readout = totals[2 * rows : 3 * rows] + totals[3 * rows :] - along * along_read + val.astype(F32) * val_read
    centred = readout - jnp.mean(readout, axis=-1, keepdims=True)
    normed_out = centred * lax.rsqrt(jnp.mean(centred * centred, axis=-1, keepdims=True) + group_eps)
    normed_out = dot(turn_back, (normed_out * of_heads(1)).astype(BF16)).astype(BF16)
    for h in range(heads):
        read_send[:, h * HEAD_DIM : (h + 1) * HEAD_DIM] = normed_out[h * seqs : (h + 1) * seqs, :]
    keep(read_send, read_all.at[member], recv_sem.at[4])

    def send_read(i):
        send(read_send, read_all.at[member], 4, base + member_at(i), mine)

    loop(1, plane, send_read)

    decay_w, unit_rate, key_rate = wide(decay), wide(unit * rate), wide(key * rate)
    along_high, along_low = split(along)
    spread_rows = jnp.concatenate([along_high, along_low, val], axis=0)

    def update(i):
        for k in range(2):
            block = pl.ds(pl.multiple_of((i * 2 + k) * WIDE, WIDE), WIDE)
            wider = dot(spread_rows, pick_all[:, block])
            old = state[:, :, block].reshape(rows, WIDE)
            new = old * decay_w - (wider[:rows] + wider[rows : 2 * rows]) * unit_rate
            new += wider[2 * rows :] * key_rate
            new_state[:, :, block] = new.reshape(seqs, heads, WIDE)

    loop(0, HEAD_DIM // per // 2, update)

    arrive(out_all, recv_sem.at[2])
    arrive(read_all, recv_sem.at[4])
    part = dot_t(
        read_all[...].reshape(plane * seqs, quarter), out_all[...].reshape(n_z * out_cols, quarter)
    )
    part_send[...] = part.astype(BF16).reshape(plane, seqs, n_z * out_cols)
    keep(part_send.at[member], part_all.at[mine * plane + member], recv_sem.at[5])

    def send_part(i):
        to = member_at(lax.rem(i, plane))
        send(part_send.at[to], part_all.at[mine * plane + member], 5, base + to, tp_at(i // plane))

    loop(1, plane * n_tp, send_part)

    arrive(part_all, recv_sem.at[5])
    for g in range(plane):
        total = part_all[g].astype(F32)
        for t in range(1, n_tp):
            total += part_all[t * plane + g].astype(F32)
        for z in range(n_z):
            at = (z * plane + g) * out_cols
            mix_rows[:, at : at + out_cols] = total[:, z * out_cols : (z + 1) * out_cols]
    middle = (layer_in[...].astype(F32) + rms_scale(mix_rows[...], post_gain[...])).astype(BF16)
    mix_rows[...] = middle.astype(F32)
    ffn_in = rms_scale(mix_rows[...], ffn_gain[...])

    mix_rows[...] = ffn_in
    opposite = tp_at(n_tp // 2)

    def to_slabs(values, dst):
        for s in range(CAP):
            for t in range(tiles):
                wide_rows[pl.ds(s * tiles + t, n_ep, stride=slab), :] = values[s][:, t * LANES : (t + 1) * LANES]
        dst[...] = wide_rows[...].astype(BF16).reshape(n_ep, slab, LANES)

    def to_everyone(src, dst, phase):
        keep(src.at[me], dst.at[me], recv_sem.at[phase])

        others(lambda to: send(src.at[to], dst.at[me], phase, to, mine))

    for at, src, dst, phase in ((mine, slot_send, slot_here, 6), (opposite, slot_far_send, slot_far, 11)):
        cut = mix_rows[:, pl.ds(pl.multiple_of(at * quarter, quarter), quarter)].astype(BF16)
        to_slabs(
            [dot(jnp.where(before_t == float(s), named_t, 0.0).astype(BF16), cut) for s in range(CAP)], src
        )
        to_everyone(src, dst, phase)
    mix_rows[...] = middle.astype(F32)

    arrive(slot_here, recv_sem.at[6])
    sides = (1, n_tp - 1)
    for step in sides:
        send(slot_here, slot_all.at[mine], 7, me, tp_at(step), slot_sem.at[mine])
    loads[first_big + 1].wait()
    loads[first_big + 2].wait()

    def from_slabs(source):
        wide_rows[...] = source.astype(F32).reshape(n_ep * slab, LANES)
        return [
            [wide_rows[pl.ds(s * tiles + t, n_ep, stride=slab), :] for t in range(tiles)]
            for s in range(CAP)
        ]

    gate = up = None
    for step in (0, n_tp // 2) + sides:
        at = tp_at(step)
        if step == 0:
            source = slot_here[...]
        elif step == n_tp // 2:
            arrive(slot_far, recv_sem.at[11])
            source = slot_far[...]
        else:
            arrive(slot_all.at[at], slot_sem.at[at])
            source = slot_all[at]
        part = jnp.concatenate([jnp.concatenate(p, axis=1) for p in from_slabs(source)], axis=0).astype(BF16)
        feats = pl.ds(pl.multiple_of(at * quarter, quarter), quarter)
        gate_part, up_part = dot(part, w_gate[feats, :]), dot(part, w_up[feats, :])
        gate = gate_part if gate is None else gate + gate_part
        up = up_part if up is None else up + up_part
    gate = jnp.minimum(gate, clamp_limit)
    up = jnp.clip(up, -clamp_limit, clamp_limit)
    hidden = ((up + 1.0) * gate * jax.nn.sigmoid(gate_alpha * gate)).astype(BF16)

    loads[first_big + 3].wait()

    def down(at):
        return dot(hidden, w_down[:, pl.ds(pl.multiple_of(at * quarter, quarter), quarter)]).astype(BF16)

    def slabs_back(values, src, dst, phase):
        to_slabs([values[s * n_ep : (s + 1) * n_ep] for s in range(CAP)], src)
        to_everyone(src, dst, phase)

    for step in sides:
        at = tp_at(step)
        down_send[at] = down(at)
        send(down_send.at[at], down_all.at[mine], 8, me, at, slot_sem.at[n_tp + mine])
    slabs_back(down(opposite).astype(F32), back_far_send, back_far, 12)
    total = down(mine).astype(F32)
    for step in sides:
        at = tp_at(step)
        arrive(down_all.at[at], slot_sem.at[n_tp + at])
        total += down_all[at].astype(F32)
    slabs_back(total, back_send, back_all, 9)

    for n, (buffer, phase) in enumerate(((back_far, 12), (back_all, 9))):
        arrive(buffer, recv_sem.at[phase])
        moe = jnp.zeros((seqs, quarter), F32)
        for (high, low), p in zip(combine, from_slabs(buffer[...])):
            values = jnp.concatenate(p, axis=1).astype(BF16)
            moe += dot(high, values) + dot(low, values)
        moe_send[n] = moe.astype(BF16)
        last = 14 if n == 0 else 10
        keep(moe_send.at[n], moe_all.at[n, mine], recv_sem.at[last])
        for step in range(1, n_tp):
            send(moe_send.at[n], moe_all.at[n, mine], last, me, tp_at(step))
    arrive(moe_all.at[0], recv_sem.at[14])
    arrive(moe_all.at[1], recv_sem.at[10])
    moe = jnp.concatenate(
        [moe_all[1, t].astype(F32) + moe_all[0, (t + n_tp // 2) % n_tp].astype(F32) for t in range(n_tp)], axis=1
    )
    layer_out[...] = (mix_rows[...] + rms_scale(moe, out_gain[...])).astype(BF16)

    sent(rows_all.at[pl.ds(0, plane // 2 - 1), 0], 0)
    sent(rows_all.at[:, core], 13)
    sent(moe_all.at[0, pl.ds(0, n_tp - 1)], 14)
    sent(proj_all.at[pl.ds(0, n_ep - 1)], 1)
    sent(out_all.at[pl.ds(0, n_z - 1)], 2)
    sent(slot_far.at[pl.ds(0, n_ep - 1)], 11)
    sent(back_far.at[pl.ds(0, n_ep - 1)], 12)
    sent(qkv_all.at[pl.ds(0, plane - 1)], 3)
    sent(read_all.at[pl.ds(0, plane - 1)], 4)
    sent(part_all.at[pl.ds(0, n_tp * plane - 1)], 5)
    sent(slot_here.at[pl.ds(0, n_ep - 1)], 6)
    sent(slot_all.at[pl.ds(0, 2)], 7)
    sent(down_all.at[pl.ds(0, 2)], 8)
    sent(back_all.at[pl.ds(0, n_ep - 1)], 9)
    sent(moe_all.at[1, pl.ds(0, n_tp - 1)], 10)


def local(n_ep, n_tp, *args):
    (
        layer_in,
        state_in,
        mix_gain,
        rec_weight,
        key_weight,
        val_weight,
        decay_down,
        decay_up,
        decay_base,
        rate_down,
        rate_up,
        rate_base,
        key_scale,
        group_gain,
        out_weight,
        post_gain,
        ffn_gain,
        routes,
        route_gates,
        expert_gate,
        expert_up,
        expert_down,
        out_gain,
    ) = args
    seqs, width = layer_in.shape
    heads = state_in.shape[1]
    plane = heads
    n_z = n_ep // plane
    quarter = width // n_tp
    slab = CAP * (quarter // LANES)
    depth = rec_weight.shape[0]
    out_cols = out_weight.shape[1]
    slots = CAP * n_ep
    state_lanes = state_in.shape[2]
    row = lambda a: a.reshape(1, -1)
    operands = (
        layer_in,
        rec_weight,
        key_weight,
        val_weight,
        out_weight.T,
        row(mix_gain),
        decay_down.T,
        rate_down.T,
        decay_up,
        rate_up,
        row(decay_base),
        row(rate_base),
        row(key_scale),
        row(group_gain),
        routes.T,
        route_gates.T,
        row(post_gain),
        row(ffn_gain),
        row(out_gain),
        state_in,
        expert_gate,
        expert_up,
        expert_down,
    )
    far = pl.BlockSpec(memory_space=pltpu.HBM)
    local_shapes = [a.shape[1:] if a.ndim == 3 and n >= len(operands) - 3 else a.shape for n, a in enumerate(operands)]
    scratch = [pltpu.VMEM(shape, a.dtype) for shape, a in zip(local_shapes, operands)]
    scratch += [
        pltpu.VMEM((plane, depth + depth // 2, 2 * HEAD_DIM), BF16),
        pltpu.VMEM((n_ep, depth + depth // 2, 2 * HEAD_DIM), BF16),
        pltpu.VMEM((n_z, out_cols, quarter), BF16),
        pltpu.VMEM((plane // 2, 2, seqs, width), BF16),
        pltpu.VMEM((plane * seqs, width), BF16),
        pltpu.VMEM((plane, seqs, WIDE), BF16),
        pltpu.VMEM((plane, seqs, WIDE), BF16),
        pltpu.VMEM((heads * seqs, HEAD_DIM), F32),
        pltpu.VMEM((heads * seqs, HEAD_DIM), F32),
        pltpu.VMEM((2, heads, HEAD_DIM), F32),
        pltpu.VMEM((HEAD_DIM * HEAD_DIM, HEAD_DIM), BF16),
        pltpu.VMEM((HEAD_DIM, HEAD_DIM * HEAD_DIM), BF16),
        pltpu.VMEM((seqs, quarter), BF16),
        pltpu.VMEM((plane, seqs, quarter), BF16),
        pltpu.VMEM((plane, seqs, n_z * out_cols), BF16),
        pltpu.VMEM((n_tp * plane, seqs, n_z * out_cols), BF16),
        pltpu.VMEM((seqs, width), F32),
        pltpu.VMEM((n_ep * slab, LANES), F32),
        pltpu.VMEM((n_ep, slab, LANES), BF16),
        pltpu.VMEM((n_ep, slab, LANES), BF16),
        pltpu.VMEM((n_ep, slab, LANES), BF16),
        pltpu.VMEM((n_ep, slab, LANES), BF16),
        pltpu.VMEM((n_tp, n_ep, slab, LANES), BF16),
        pltpu.VMEM((n_tp, slots, quarter), BF16),
        pltpu.VMEM((n_tp, slots, quarter), BF16),
        pltpu.VMEM((n_ep, slab, LANES), BF16),
        pltpu.VMEM((n_ep, slab, LANES), BF16),
        pltpu.VMEM((n_ep, slab, LANES), BF16),
        pltpu.VMEM((n_ep, slab, LANES), BF16),
        pltpu.VMEM((2, seqs, quarter), BF16),
        pltpu.VMEM((2, n_tp, seqs, quarter), BF16),
        pltpu.SemaphoreType.DMA((len(operands),)),
        pltpu.SemaphoreType.DMA((15,)),
        pltpu.SemaphoreType.DMA((15,)),
        pltpu.SemaphoreType.DMA((n_z,)),
        pltpu.SemaphoreType.DMA((2 * n_tp,)),
    ]
    return pl.pallas_call(
        functools.partial(kernel, n_ep, n_tp),
        out_shape=(
            jax.ShapeDtypeStruct(layer_in.shape, BF16),
            jax.ShapeDtypeStruct((seqs, heads, state_lanes), F32),
        ),
        in_specs=[far] * len(operands),
        out_specs=[pl.BlockSpec(memory_space=pltpu.VMEM)] * 2,
        scratch_shapes=scratch,
        compiler_params=pltpu.CompilerParams(
            collective_id=0, has_side_effects=True, vmem_limit_bytes=32 * 1024 * 1024
        ),
    )(*[pltpu.with_memory_space_constraint(a, pltpu.HBM) for a in operands])


def solution(mesh):
    in_specs = (
        P("ep", None),
        P("ep", "tp", None),
        P(),
        P("ep", "tp"),
        P("ep", "tp"),
        P("ep", "tp"),
        P(),
        P(None, "tp"),
        P("tp"),
        P(),
        P(None, "tp"),
        P("tp"),
        P("tp"),
        P("tp"),
        P("tp", "ep"),
        P(),
        P(),
        P("ep", None),
        P("ep", None),
        P("ep", None, "tp"),
        P("ep", None, "tp"),
        P("ep", "tp", None),
        P(),
    )
    out_specs = (P("ep", None), P("ep", "tp", None))
    body = functools.partial(local, mesh.shape["ep"], mesh.shape["tp"])
    return jax.shard_map(body, mesh=mesh, in_specs=in_specs, out_specs=out_specs, check_vma=False)
```

```python
import functools

import jax
import jax.numpy as jnp
from jax import lax
from jax.experimental import pallas as pl
from jax.experimental.pallas import tpu as pltpu
from jax.sharding import PartitionSpec as P

MESH = pl.DeviceIdType.MESH
HEAD_DIM = 64
CAP = 2
LANES = 128
WIDE = 256

norm_eps = 1e-06
group_eps = 0.00064
clamp_limit = 7.0
gate_alpha = 1.702

F32 = jnp.float32
BF16 = jnp.bfloat16


def dot(a, b):
    return lax.dot_general(a, b, (((1,), (0,)), ((), ())), preferred_element_type=F32)


def dot_t(a, b):
    return lax.dot_general(a, b, (((1,), (1,)), ((), ())), preferred_element_type=F32)


def split(a):
    high = a.astype(BF16)
    return high, (a - high.astype(F32)).astype(BF16)


def dot_split(a, b):
    high, low = split(a)
    return dot(high, b) + dot(low, b)


def iota(shape, dim):
    return lax.broadcasted_iota(jnp.int32, shape, dim)


def one_hot(mask):
    return jnp.where(mask, 1.0, 0.0).astype(BF16)


def rms_scale(values, scales):
    return values * lax.rsqrt(jnp.mean(values * values, axis=-1, keepdims=True) + norm_eps) * scales


def kernel(
    n_ep,
    n_tp,
    layer_in_far,
    rec_weight_far,
    key_weight_far,
    val_weight_far,
    out_weight_t_far,
    mix_gain_far,
    decay_down_t_far,
    rate_down_t_far,
    decay_up_far,
    rate_up_far,
    decay_base_far,
    rate_base_far,
    key_scale_far,
    group_gain_far,
    routes_t_far,
    gates_t_far,
    post_gain_far,
    ffn_gain_far,
    out_gain_far,
    state_far,
    expert_gate_far,
    expert_up_far,
    expert_down_far,
    layer_out,
    new_state,
    layer_in,
    rec_weight,
    key_weight,
    val_weight,
    out_send,
    mix_gain,
    decay_down_t,
    rate_down_t,
    decay_up,
    rate_up,
    decay_base,
    rate_base,
    key_scale,
    group_gain,
    routes_t,
    gates_t,
    post_gain,
    ffn_gain,
    out_gain,
    state,
    w_gate,
    w_up,
    w_down,
    pair_send,
    pair_all,
    val_send,
    val_all,
    out_all,
    rows_all,
    normed_all,
    pair_out,
    pair_in,
    val_out,
    val_in,
    decay_rows,
    rate_rows,
    by_head,
    gather_all,
    pick_all,
    read_send,
    read_all,
    part_send,
    part_all,
    mix_rows,
    wide_rows,
    slot_send,
    slot_here,
    slot_far_send,
    slot_far,
    slot_all,
    down_send,
    down_all,
    back_send,
    back_all,
    back_far_send,
    back_far,
    moe_send,
    moe_all,
    load_sem,
    send_sem,
    recv_sem,
    pair_sem,
    val_sem,
    near_sem,
    slot_sem,
    down_sem,
):
    far = (
        layer_in_far,
        rec_weight_far,
        key_weight_far,
        val_weight_far,
        out_weight_t_far,
        mix_gain_far,
        decay_down_t_far,
        rate_down_t_far,
        decay_up_far,
        rate_up_far,
        decay_base_far,
        rate_base_far,
        key_scale_far,
        group_gain_far,
        routes_t_far,
        gates_t_far,
        post_gain_far,
        ffn_gain_far,
        out_gain_far,
        state_far,
        expert_gate_far.at[0],
        expert_up_far.at[0],
        expert_down_far.at[0],
    )
    near = (
        layer_in,
        rec_weight,
        key_weight,
        val_weight,
        out_send,
        mix_gain,
        decay_down_t,
        rate_down_t,
        decay_up,
        rate_up,
        decay_base,
        rate_base,
        key_scale,
        group_gain,
        routes_t,
        gates_t,
        post_gain,
        ffn_gain,
        out_gain,
        state,
        w_gate,
        w_up,
        w_down,
    )
    loads = [pltpu.make_async_copy(a, b, load_sem.at[n]) for n, (a, b) in enumerate(zip(far, near))]
    first_big = len(loads) - 4
    seqs, width = layer_in.shape
    heads = state.shape[1]
    plane = heads
    n_z = n_ep // plane
    quarter = width // n_tp
    tiles = quarter // LANES
    slab = CAP * tiles
    rows = seqs * heads
    depth = rec_weight.shape[0]
    out_cols = out_send.shape[0]

    for load in loads[:first_big]:
        load.start()

    me = lax.axis_index("ep")
    mine = lax.axis_index("tp")
    member = lax.rem(me, plane)
    base = me - member

    def member_at(step):
        return lax.rem(member + step, plane)

    def z_at(step):
        return lax.rem(me + step * plane, n_ep)

    def tp_at(step):
        return lax.rem(mine + step, n_tp)

    def send(src, dst, phase, ep, tp, sem=None):
        pltpu.make_async_remote_copy(
            src_ref=src,
            dst_ref=dst,
            send_sem=send_sem.at[phase],
            recv_sem=recv_sem.at[phase] if sem is None else sem,
            device_id={"ep": ep, "tp": tp},
            device_id_type=MESH,
        ).start()

    def keep(src, dst, sem):
        pltpu.make_async_copy(src, dst, sem).start()

    def arrive(buffer, sem):
        pltpu.make_async_copy(buffer, buffer, sem).wait()

    def sent(buffer, phase):
        pltpu.make_async_copy(buffer, buffer, send_sem.at[phase]).wait()

    def loop(start, stop, body):
        def step(i, carry):
            body(i)
            return carry

        lax.fori_loop(start, stop, step, 0)

    barrier = pltpu.get_barrier_semaphore()

    def others(body):
        for k in range(n_z):
            away = n_z // 2 + (k + 1) // 2 * (1 if k % 2 else -1)
            first = lax.rem(base + away % n_z * plane, n_ep)
            loop(
                0 if away % n_z else 1,
                plane,
                lambda i, first=first, away=away: body(first + member_at(i), away),
            )

    def greet(to, away):
        pl.semaphore_signal(barrier, inc=1, device_id={"ep": to, "tp": mine}, device_id_type=MESH)

    others(greet)

    def greet_plane(i):
        pl.semaphore_signal(
            barrier,
            inc=1,
            device_id={"ep": base + member_at(lax.rem(i, plane)), "tp": tp_at(i // plane)},
            device_id_type=MESH,
        )

    loop(plane, plane * n_tp, greet_plane)

    for load in loads[:5]:
        load.wait()
    for h in range(heads):
        cut = slice(h * HEAD_DIM, (h + 1) * HEAD_DIM)
        pair_send[h] = jnp.concatenate([rec_weight[:, cut], key_weight[:, cut]], axis=1)
        val_send[h] = jnp.concatenate(
            [val_weight[: depth // 2, cut], val_weight[depth // 2 :, cut]], axis=1
        )
    for load in loads[first_big:]:
        load.start()
    for load in loads[5:first_big]:
        load.wait()
    pl.semaphore_wait(barrier, n_ep - 1 + plane * (n_tp - 1))

    keep(pair_send.at[member], pair_all.at[me], pair_sem.at[0])
    keep(val_send.at[member], val_all.at[me], val_sem.at[0])
    pair_wave = (pair_send, pair_all, 1, pair_sem)
    val_wave = (val_send, val_all, 15, val_sem)

    def send_wave(wave, away):
        src, dst, phase, sem = wave
        first = lax.rem(base + away % n_z * plane, n_ep)

        def one(i):
            to = member_at(i)
            send(src.at[to], dst.at[me], phase, first + to, mine, sem.at[-away % n_z])

        loop(0 if away else 1, plane, one)

    for away in (2, -2):
        send_wave(pair_wave, away)
    chip, core = member // 2, lax.rem(member, 2)
    keep(layer_in, rows_all.at[chip, core], recv_sem.at[0])

    def send_rows(i):
        send(layer_in, rows_all.at[chip, core], 0, base + member_at(2 * i), mine)

    loop(1, plane // 2, send_rows)
    for away in (1, -1, 0):
        send_wave(pair_wave, away)
    for away in (2, -2):
        send_wave(val_wave, away)
    z_me = me // plane

    own_normed = rms_scale(layer_in[...].astype(F32), mix_gain[...]).astype(BF16)
    decay_hidden = jnp.tanh(dot_t(own_normed, decay_down_t[...])).astype(BF16)
    rate_hidden = dot_t(own_normed, rate_down_t[...]).astype(BF16)
    decay_sig = jax.nn.sigmoid(decay_base[...] + dot(decay_hidden, decay_up[...]))
    decay = jnp.exp(-jnp.exp(jnp.full((), -0.5, F32)) * decay_sig)
    rate = jax.nn.sigmoid(rate_base[...] + dot(rate_hidden, rate_up[...]))
    for h in range(heads):
        cut = slice(h * HEAD_DIM, (h + 1) * HEAD_DIM)
        decay_rows[h * seqs : (h + 1) * seqs, :] = decay[:, cut]
        rate_rows[h * seqs : (h + 1) * seqs, :] = rate[:, cut]
        by_head[0, h : h + 1, :] = key_scale[:, cut]
        by_head[1, h : h + 1, :] = group_gain[:, cut]

    top = routes_t.shape[0]
    named_t = jnp.zeros((n_ep, seqs), F32)
    weight_t = jnp.zeros((n_ep, seqs), F32)
    for j in range(top):
        hit = iota((n_ep, seqs), 0) == routes_t[j : j + 1, :]
        named_t += jnp.where(hit, 1.0, 0.0)
        weight_t += jnp.where(hit, gates_t[j : j + 1, :], 0.0)
    before_t = dot(named_t.astype(BF16), one_hot(iota((seqs, seqs), 0) < iota((seqs, seqs), 1)))
    eye = one_hot(iota((seqs, seqs), 0) == iota((seqs, seqs), 1))
    combine = []
    for s in range(CAP):
        high, low = split(jnp.where(before_t == float(s), weight_t, 0.0))
        combine.append((dot_t(eye, high).astype(BF16), dot_t(eye, low).astype(BF16)))
    per = WIDE // HEAD_DIM

    def tables(i):
        block = pl.ds(pl.multiple_of(i * WIDE, WIDE), WIDE)
        pick_all[:, block] = one_hot(
            iota((HEAD_DIM, WIDE), 0) == i * per + iota((HEAD_DIM, WIDE), 1) // HEAD_DIM
        )
        gather_all[block, :] = one_hot(
            iota((WIDE, HEAD_DIM), 1) == i * per + iota((WIDE, HEAD_DIM), 0) // HEAD_DIM
        )

    loop(0, HEAD_DIM // per, tables)

    def plane_of(buffer, away):
        at = lax.rem(base + away % n_z * plane, n_ep)
        return at, buffer.at[pl.ds(at, plane)]

    half = plane // 2

    def forward(wave):
        _, buffer, phase, sem = wave
        for away in (-2, 2):
            at, blocks = plane_of(buffer, away)
            arrive(blocks, sem.at[away % n_z])
            side = -away // 2
            to = lax.rem(base + side % n_z * plane, n_ep) + member
            send(blocks, blocks, phase, to, mine, sem.at[(away - side) % n_z])
            part = buffer.at[pl.ds(at + (0 if side > 0 else half), half)]
            to = lax.rem(base + 2 * side % n_z * plane, n_ep) + member
            send(part, part, phase, to, mine, sem.at[(away - 2 * side) % n_z])

    def arrive_wave(wave):
        _, buffer, _, sem = wave
        for away in (0, 1, -1, 3, -3, 4):
            arrive(plane_of(buffer, away)[1], sem.at[away % n_z])

    forward(pair_wave)
    for away in (1, -1, 0):
        send_wave(val_wave, away)
    arrive(rows_all.at[:, core], recv_sem.at[0])
    sibling = me + 1 - 2 * core
    send(rows_all.at[:, core], rows_all.at[:, core], 13, sibling, mine)
    forward(val_wave)
    keep(out_send, out_all.at[z_me], recv_sem.at[2])

    def send_out(i):
        send(out_send, out_all.at[z_me], 2, z_at(i), mine)

    loop(1, n_z, send_out)

    arrive(rows_all.at[:, 1 - core], recv_sem.at[13])

    def norm_rows(i):
        values = rms_scale(rows_all[i // 2, lax.rem(i, 2)].astype(F32), mix_gain[...]).astype(BF16)
        normed_all[pl.ds(pl.multiple_of(i * seqs, seqs), seqs), :] = values

    loop(0, plane, norm_rows)

    arrive_wave(pair_wave)
    normed = normed_all[...]
    pair_sum = dot(normed, pair_all[...].reshape(n_ep * depth, 2 * HEAD_DIM))
    pair_out[...] = pair_sum.astype(BF16).reshape(plane, seqs, 2 * HEAD_DIM)

    def share(src, dst, phase):
        keep(src.at[member], dst.at[member], recv_sem.at[phase])

        def one(i):
            to = member_at(i)
            send(src.at[to], dst.at[member], phase, base + to, mine)

        loop(1, plane, one)

    share(pair_out, pair_in, 3)

    arrive_wave(val_wave)
    vals = val_all[...]
    vals = jnp.concatenate([vals, vals], axis=1).reshape(n_ep * depth, 2 * HEAD_DIM)
    spread = (n_ep * depth, 2 * HEAD_DIM)
    first = lax.rem(iota(spread, 0), depth) < depth // 2
    vals = jnp.where(first == (iota(spread, 1) < HEAD_DIM), vals.astype(F32), 0.0).astype(BF16)
    val_sum = dot(normed, vals)
    val_sum = val_sum[:, :HEAD_DIM] + val_sum[:, HEAD_DIM:]
    val_sum = jnp.concatenate([val_sum, jnp.zeros_like(val_sum)], axis=1)
    val_out[...] = val_sum.astype(BF16).reshape(plane, seqs, 2 * HEAD_DIM)
    share(val_out, val_in, 16)

    turn = one_hot(
        iota((rows, rows), 1)
        == lax.rem(iota((rows, rows), 0), heads) * seqs + iota((rows, rows), 0) // heads
    )
    turn_back = one_hot(
        iota((rows, rows), 1)
        == lax.rem(iota((rows, rows), 0), seqs) * heads + iota((rows, rows), 0) // seqs
    )
    decay_high, decay_low = split(decay_rows[...])
    rate_high, rate_low = split(rate_rows[...])
    turned = dot(turn, jnp.concatenate([decay_high, decay_low, rate_high, rate_low], axis=1))
    decay = turned[:, :HEAD_DIM] + turned[:, HEAD_DIM : 2 * HEAD_DIM]
    rate = turned[:, 2 * HEAD_DIM : 3 * HEAD_DIM] + turned[:, 3 * HEAD_DIM :]

    arrive(pair_in, recv_sem.at[3])
    pair = dot(turn, pair_in[...].reshape(rows, 2 * HEAD_DIM))
    rec = pair[:, :HEAD_DIM]
    key = pair[:, HEAD_DIM:]

    def of_heads(n):
        return jnp.broadcast_to(by_head[n][None], (seqs, heads, HEAD_DIM)).reshape(rows, HEAD_DIM)

    scaled = key * of_heads(0)
    unit = scaled * lax.rsqrt(jnp.sum(scaled * scaled, axis=-1, keepdims=True) + norm_eps)

    def wide(a):
        return jnp.concatenate([a] * (WIDE // HEAD_DIM), axis=1)

    unit_w, read_w = wide(unit), wide(decay * rec)
    loads[first_big].wait()

    def sums(i, totals):
        for k in range(4):
            block = pl.ds(pl.multiple_of((i * 4 + k) * WIDE, WIDE), WIDE)
            old = state[:, :, block].reshape(rows, WIDE)
            stacked = jnp.concatenate(split(old * unit_w) + split(old * read_w), axis=0)
            totals += dot(stacked, gather_all[block, :])
        return totals

    totals = lax.fori_loop(0, HEAD_DIM // per // 4, sums, jnp.zeros((4 * rows, HEAD_DIM), F32))
    along = totals[:rows] + totals[rows : 2 * rows]
    along_read = jnp.sum(unit * rate * rec, axis=-1, keepdims=True)
    val_read = jnp.sum(key * rate * rec, axis=-1, keepdims=True)
    arrive(val_in, recv_sem.at[16])
    val = dot(turn, val_in[...].reshape(rows, 2 * HEAD_DIM))[:, :HEAD_DIM].astype(BF16)
    readout = totals[2 * rows : 3 * rows] + totals[3 * rows :] - along * along_read + val.astype(F32) * val_read
    centred = readout - jnp.mean(readout, axis=-1, keepdims=True)
    normed_out = centred * lax.rsqrt(jnp.mean(centred * centred, axis=-1, keepdims=True) + group_eps)
    normed_out = dot(turn_back, (normed_out * of_heads(1)).astype(BF16)).astype(BF16)
    for h in range(heads):
        read_send[:, h * HEAD_DIM : (h + 1) * HEAD_DIM] = normed_out[h * seqs : (h + 1) * seqs, :]
    keep(read_send, read_all.at[member], recv_sem.at[4])

    def send_read(i):
        send(read_send, read_all.at[member], 4, base + member_at(i), mine)

    loop(1, plane, send_read)

    decay_w, unit_rate, key_rate = wide(decay), wide(unit * rate), wide(key * rate)
    along_high, along_low = split(along)
    spread_rows = jnp.concatenate([along_high, along_low, val], axis=0)

    def update(i):
        for k in range(2):
            block = pl.ds(pl.multiple_of((i * 2 + k) * WIDE, WIDE), WIDE)
            wider = dot(spread_rows, pick_all[:, block])
            old = state[:, :, block].reshape(rows, WIDE)
            new = old * decay_w - (wider[:rows] + wider[rows : 2 * rows]) * unit_rate
            new += wider[2 * rows :] * key_rate
            new_state[:, :, block] = new.reshape(seqs, heads, WIDE)

    loop(0, HEAD_DIM // per // 2, update)

    arrive(out_all, recv_sem.at[2])
    arrive(read_all, recv_sem.at[4])
    part = dot_t(
        read_all[...].reshape(plane * seqs, quarter), out_all[...].reshape(n_z * out_cols, quarter)
    )
    part_send[...] = part.astype(BF16).reshape(plane, seqs, n_z * out_cols)
    keep(part_send.at[member], part_all.at[mine * plane + member], recv_sem.at[5])

    def send_part(i):
        to = member_at(lax.rem(i, plane))
        send(part_send.at[to], part_all.at[mine * plane + member], 5, base + to, tp_at(i // plane))

    loop(1, plane * n_tp, send_part)

    arrive(part_all, recv_sem.at[5])
    for g in range(plane):
        total = part_all[g].astype(F32)
        for t in range(1, n_tp):
            total += part_all[t * plane + g].astype(F32)
        for z in range(n_z):
            at = (z * plane + g) * out_cols
            mix_rows[:, at : at + out_cols] = total[:, z * out_cols : (z + 1) * out_cols]
    middle = (layer_in[...].astype(F32) + rms_scale(mix_rows[...], post_gain[...])).astype(BF16)
    mix_rows[...] = middle.astype(F32)
    ffn_in = rms_scale(mix_rows[...], ffn_gain[...])

    mix_rows[...] = ffn_in
    opposite = tp_at(n_tp // 2)

    def to_slabs(values, dst):
        for s in range(CAP):
            for t in range(tiles):
                wide_rows[pl.ds(s * tiles + t, n_ep, stride=slab), :] = values[s][:, t * LANES : (t + 1) * LANES]
        dst[...] = wide_rows[...].astype(BF16).reshape(n_ep, slab, LANES)

    def to_everyone(src, dst, phase, sems=None):
        def sem_of(away):
            return recv_sem.at[phase] if sems is None else sems.at[-away % n_z]

        keep(src.at[me], dst.at[me], sem_of(0))
        others(lambda to, away: send(src.at[to], dst.at[me], phase, to, mine, sem_of(away)))

    for at, src, dst, phase, sems in (
        (mine, slot_send, slot_here, 6, near_sem),
        (opposite, slot_far_send, slot_far, 11, None),
    ):
        cut = mix_rows[:, pl.ds(pl.multiple_of(at * quarter, quarter), quarter)].astype(BF16)
        to_slabs(
            [dot(jnp.where(before_t == float(s), named_t, 0.0).astype(BF16), cut) for s in range(CAP)], src
        )
        to_everyone(src, dst, phase, sems)
    mix_rows[...] = middle.astype(F32)

    sides = (1, n_tp - 1)
    for away in (0, 1, -1, 2, -2, 3, -3, 4):
        at, blocks = plane_of(slot_here, away)
        arrive(blocks, near_sem.at[away % n_z])
        for step in sides:
            send(blocks, slot_all.at[mine, pl.ds(at, plane)], 7, me, tp_at(step), slot_sem.at[mine])
    loads[first_big + 1].wait()
    loads[first_big + 2].wait()

    def from_slabs(source):
        wide_rows[...] = source.astype(F32).reshape(n_ep * slab, LANES)
        return [
            [wide_rows[pl.ds(s * tiles + t, n_ep, stride=slab), :] for t in range(tiles)]
            for s in range(CAP)
        ]

    gate = up = None
    for step in (0, n_tp // 2) + sides:
        at = tp_at(step)
        if step == 0:
            source = slot_here[...]
        elif step == n_tp // 2:
            arrive(slot_far, recv_sem.at[11])
            source = slot_far[...]
        else:
            arrive(slot_all.at[at], slot_sem.at[at])
            source = slot_all[at]
        part = jnp.concatenate(
            [jnp.concatenate(p, axis=1).reshape(n_z, 1, plane, quarter) for p in from_slabs(source)], axis=1
        )
        part = part.reshape(n_ep * CAP, quarter).astype(BF16)
        feats = pl.ds(pl.multiple_of(at * quarter, quarter), quarter)
        gate_part, up_part = dot(part, w_gate[feats, :]), dot(part, w_up[feats, :])
        gate = gate_part if gate is None else gate + gate_part
        up = up_part if up is None else up + up_part
    gate = jnp.minimum(gate, clamp_limit)
    up = jnp.clip(up, -clamp_limit, clamp_limit)
    hidden = ((up + 1.0) * gate * jax.nn.sigmoid(gate_alpha * gate)).astype(BF16)

    loads[first_big + 3].wait()

    def down(at):
        return dot(hidden, w_down[:, pl.ds(pl.multiple_of(at * quarter, quarter), quarter)]).astype(BF16)

    planes = [n_z // 2 + (k + 1) // 2 * (1 if k % 2 else -1) for k in range(n_z)]

    def block_of(away):
        at = lax.rem(base + away % n_z * plane, n_ep)
        return at, pl.ds(pl.multiple_of(at * CAP, plane * CAP), plane * CAP)

    for side, step in enumerate(sides):
        at = tp_at(step)
        down_send[at] = down(at)
        for away in planes:
            block = block_of(away)[1]
            send(
                down_send.at[at, block],
                down_all.at[mine, block],
                8,
                me,
                at,
                down_sem.at[side * n_z + away % n_z],
            )
    values = down(opposite).astype(F32).reshape(n_z, CAP, plane, quarter)
    to_slabs([values[:, s].reshape(n_ep, quarter) for s in range(CAP)], back_far_send)
    to_everyone(back_far_send, back_far, 12)
    down_all[mine] = down(mine)

    for away in planes:
        at, block = block_of(away)
        total = down_all[mine, block].astype(F32)
        for side, step in enumerate(sides):
            source = tp_at(n_tp - step)
            arrive(down_all.at[source, block], down_sem.at[side * n_z + away % n_z])
            total += down_all[source, block].astype(F32)
        for s in range(CAP):
            for t in range(tiles):
                wide_rows[pl.ds(at * slab + s * tiles + t, plane, stride=slab), :] = total[
                    s * plane : (s + 1) * plane, t * LANES : (t + 1) * LANES
                ]
        slabs = wide_rows[pl.ds(pl.multiple_of(at * slab, plane * slab), plane * slab), :]
        back_send[pl.ds(at, plane)] = slabs.astype(BF16).reshape(plane, slab, LANES)

        def send_back(i, at=at):
            to = at + member_at(i)
            send(back_send.at[to], back_all.at[me], 9, to, mine)

        if away % n_z == 0:
            keep(back_send.at[me], back_all.at[me], recv_sem.at[9])
        loop(0 if away % n_z else 1, plane, send_back)

    for n, (buffer, phase) in enumerate(((back_far, 12), (back_all, 9))):
        arrive(buffer, recv_sem.at[phase])
        moe = jnp.zeros((seqs, quarter), F32)
        for (high, low), p in zip(combine, from_slabs(buffer[...])):
            values = jnp.concatenate(p, axis=1).astype(BF16)
            moe += dot(high, values) + dot(low, values)
        moe_send[n] = moe.astype(BF16)
        last = 14 if n == 0 else 10
        keep(moe_send.at[n], moe_all.at[n, mine], recv_sem.at[last])
        for step in range(1, n_tp):
            send(moe_send.at[n], moe_all.at[n, mine], last, me, tp_at(step))
    arrive(moe_all.at[0], recv_sem.at[14])
    arrive(moe_all.at[1], recv_sem.at[10])
    moe = jnp.concatenate(
        [moe_all[1, t].astype(F32) + moe_all[0, (t + n_tp // 2) % n_tp].astype(F32) for t in range(n_tp)], axis=1
    )
    layer_out[...] = (mix_rows[...] + rms_scale(moe, out_gain[...])).astype(BF16)

    sent(rows_all.at[pl.ds(0, plane // 2 - 1), 0], 0)
    sent(rows_all.at[:, core], 13)
    sent(moe_all.at[0, pl.ds(0, n_tp - 1)], 14)
    sent(pair_all.at[pl.ds(0, n_ep - 1)], 1)
    sent(val_all.at[pl.ds(0, n_ep - 1)], 15)
    sent(out_all.at[pl.ds(0, n_z - 1)], 2)
    sent(slot_far.at[pl.ds(0, n_ep - 1)], 11)
    sent(back_far.at[pl.ds(0, n_ep - 1)], 12)
    sent(pair_in.at[pl.ds(0, plane - 1)], 3)
    sent(val_in.at[pl.ds(0, plane - 1)], 16)
    sent(read_all.at[pl.ds(0, plane - 1)], 4)
    sent(part_all.at[pl.ds(0, n_tp * plane - 1)], 5)
    sent(slot_here.at[pl.ds(0, n_ep - 1)], 6)
    sent(slot_all.at[pl.ds(0, 2)], 7)
    sent(down_all.at[pl.ds(0, 2)], 8)
    sent(back_all.at[pl.ds(0, n_ep - 1)], 9)
    sent(moe_all.at[1, pl.ds(0, n_tp - 1)], 10)


def local(n_ep, n_tp, *args):
    (
        layer_in,
        state_in,
        mix_gain,
        rec_weight,
        key_weight,
        val_weight,
        decay_down,
        decay_up,
        decay_base,
        rate_down,
        rate_up,
        rate_base,
        key_scale,
        group_gain,
        out_weight,
        post_gain,
        ffn_gain,
        routes,
        route_gates,
        expert_gate,
        expert_up,
        expert_down,
        out_gain,
    ) = args
    seqs, width = layer_in.shape
    heads = state_in.shape[1]
    plane = heads
    n_z = n_ep // plane
    quarter = width // n_tp
    slab = CAP * (quarter // LANES)
    depth = rec_weight.shape[0]
    out_cols = out_weight.shape[1]
    slots = CAP * n_ep
    state_lanes = state_in.shape[2]
    row = lambda a: a.reshape(1, -1)
    operands = (
        layer_in,
        rec_weight,
        key_weight,
        val_weight,
        out_weight.T,
        row(mix_gain),
        decay_down.T,
        rate_down.T,
        decay_up,
        rate_up,
        row(decay_base),
        row(rate_base),
        row(key_scale),
        row(group_gain),
        routes.T,
        route_gates.T,
        row(post_gain),
        row(ffn_gain),
        row(out_gain),
        state_in,
        expert_gate,
        expert_up,
        expert_down,
    )
    far = pl.BlockSpec(memory_space=pltpu.HBM)
    local_shapes = [a.shape[1:] if a.ndim == 3 and n >= len(operands) - 3 else a.shape for n, a in enumerate(operands)]
    scratch = [pltpu.VMEM(shape, a.dtype) for shape, a in zip(local_shapes, operands)]
    scratch += [
        pltpu.VMEM((plane, depth, 2 * HEAD_DIM), BF16),
        pltpu.VMEM((n_ep, depth, 2 * HEAD_DIM), BF16),
        pltpu.VMEM((plane, depth // 2, 2 * HEAD_DIM), BF16),
        pltpu.VMEM((n_ep, depth // 2, 2 * HEAD_DIM), BF16),
        pltpu.VMEM((n_z, out_cols, quarter), BF16),
        pltpu.VMEM((plane // 2, 2, seqs, width), BF16),
        pltpu.VMEM((plane * seqs, width), BF16),
        pltpu.VMEM((plane, seqs, 2 * HEAD_DIM), BF16),
        pltpu.VMEM((plane, seqs, 2 * HEAD_DIM), BF16),
        pltpu.VMEM((plane, seqs, 2 * HEAD_DIM), BF16),
        pltpu.VMEM((plane, seqs, 2 * HEAD_DIM), BF16),
        pltpu.VMEM((heads * seqs, HEAD_DIM), F32),
        pltpu.VMEM((heads * seqs, HEAD_DIM), F32),
        pltpu.VMEM((2, heads, HEAD_DIM), F32),
        pltpu.VMEM((HEAD_DIM * HEAD_DIM, HEAD_DIM), BF16),
        pltpu.VMEM((HEAD_DIM, HEAD_DIM * HEAD_DIM), BF16),
        pltpu.VMEM((seqs, quarter), BF16),
        pltpu.VMEM((plane, seqs, quarter), BF16),
        pltpu.VMEM((plane, seqs, n_z * out_cols), BF16),
        pltpu.VMEM((n_tp * plane, seqs, n_z * out_cols), BF16),
        pltpu.VMEM((seqs, width), F32),
        pltpu.VMEM((n_ep * slab, LANES), F32),
        pltpu.VMEM((n_ep, slab, LANES), BF16),
        pltpu.VMEM((n_ep, slab, LANES), BF16),
        pltpu.VMEM((n_ep, slab, LANES), BF16),
        pltpu.VMEM((n_ep, slab, LANES), BF16),
        pltpu.VMEM((n_tp, n_ep, slab, LANES), BF16),
        pltpu.VMEM((n_tp, slots, quarter), BF16),
        pltpu.VMEM((n_tp, slots, quarter), BF16),
        pltpu.VMEM((n_ep, slab, LANES), BF16),
        pltpu.VMEM((n_ep, slab, LANES), BF16),
        pltpu.VMEM((n_ep, slab, LANES), BF16),
        pltpu.VMEM((n_ep, slab, LANES), BF16),
        pltpu.VMEM((2, seqs, quarter), BF16),
        pltpu.VMEM((2, n_tp, seqs, quarter), BF16),
        pltpu.SemaphoreType.DMA((len(operands),)),
        pltpu.SemaphoreType.DMA((17,)),
        pltpu.SemaphoreType.DMA((17,)),
        pltpu.SemaphoreType.DMA((n_z,)),
        pltpu.SemaphoreType.DMA((n_z,)),
        pltpu.SemaphoreType.DMA((n_z,)),
        pltpu.SemaphoreType.DMA((n_tp,)),
        pltpu.SemaphoreType.DMA((2 * n_z,)),
    ]
    return pl.pallas_call(
        functools.partial(kernel, n_ep, n_tp),
        out_shape=(
            jax.ShapeDtypeStruct(layer_in.shape, BF16),
            jax.ShapeDtypeStruct((seqs, heads, state_lanes), F32),
        ),
        in_specs=[far] * len(operands),
        out_specs=[pl.BlockSpec(memory_space=pltpu.VMEM)] * 2,
        scratch_shapes=scratch,
        compiler_params=pltpu.CompilerParams(
            collective_id=0, has_side_effects=True, vmem_limit_bytes=32 * 1024 * 1024
        ),
    )(*[pltpu.with_memory_space_constraint(a, pltpu.HBM) for a in operands])


def solution(mesh):
    in_specs = (
        P("ep", None),
        P("ep", "tp", None),
        P(),
        P("ep", "tp"),
        P("ep", "tp"),
        P("ep", "tp"),
        P(),
        P(None, "tp"),
        P("tp"),
        P(),
        P(None, "tp"),
        P("tp"),
        P("tp"),
        P("tp"),
        P("tp", "ep"),
        P(),
        P(),
        P("ep", None),
        P("ep", None),
        P("ep", None, "tp"),
        P("ep", None, "tp"),
        P("ep", "tp", None),
        P(),
    )
    out_specs = (P("ep", None), P("ep", "tp", None))
    body = functools.partial(local, mesh.shape["ep"], mesh.shape["tp"])
    return jax.shard_map(body, mesh=mesh, in_specs=in_specs, out_specs=out_specs, check_vma=False)
```

```python
import functools

import jax
import jax.numpy as jnp
from jax import lax
from jax.experimental import pallas as pl
from jax.experimental.pallas import tpu as pltpu
from jax.sharding import PartitionSpec as P

MESH = pl.DeviceIdType.MESH
HEAD_DIM = 64
CAP = 2
LANES = 128
WIDE = 256

norm_eps = 1e-06
group_eps = 0.00064
clamp_limit = 7.0
gate_alpha = 1.702

F32 = jnp.float32
BF16 = jnp.bfloat16


def dot(a, b):
    return lax.dot_general(a, b, (((1,), (0,)), ((), ())), preferred_element_type=F32)


def dot_t(a, b):
    return lax.dot_general(a, b, (((1,), (1,)), ((), ())), preferred_element_type=F32)


def split(a):
    high = a.astype(BF16)
    return high, (a - high.astype(F32)).astype(BF16)


def dot_split(a, b):
    high, low = split(a)
    return dot(high, b) + dot(low, b)


def iota(shape, dim):
    return lax.broadcasted_iota(jnp.int32, shape, dim)


def one_hot(mask):
    return jnp.where(mask, 1.0, 0.0).astype(BF16)


def rms_scale(values, scales):
    return values * lax.rsqrt(jnp.mean(values * values, axis=-1, keepdims=True) + norm_eps) * scales


def kernel(
    n_ep,
    n_tp,
    layer_in_far,
    rec_weight_far,
    key_weight_far,
    val_weight_far,
    out_weight_t_far,
    mix_gain_far,
    decay_down_t_far,
    rate_down_t_far,
    decay_up_far,
    rate_up_far,
    decay_base_far,
    rate_base_far,
    key_scale_far,
    group_gain_far,
    routes_t_far,
    gates_t_far,
    post_gain_far,
    ffn_gain_far,
    out_gain_far,
    state_far,
    expert_gate_far,
    expert_up_far,
    expert_down_far,
    layer_out,
    new_state,
    layer_in,
    rec_weight,
    key_weight,
    val_weight,
    out_send,
    mix_gain,
    decay_down_t,
    rate_down_t,
    decay_up,
    rate_up,
    decay_base,
    rate_base,
    key_scale,
    group_gain,
    routes_t,
    gates_t,
    post_gain,
    ffn_gain,
    out_gain,
    state,
    w_gate,
    w_up,
    w_down,
    pair_send,
    pair_all,
    val_send,
    val_all,
    out_all,
    rows_all,
    normed_all,
    pair_out,
    pair_in,
    val_out,
    val_in,
    decay_rows,
    rate_rows,
    by_head,
    gather_all,
    pick_all,
    read_send,
    read_all,
    part_send,
    part_all,
    mix_rows,
    wide_rows,
    slot_send,
    slot_here,
    slot_far_send,
    slot_far,
    slot_all,
    down_send,
    down_all,
    back_send,
    back_all,
    back_far_send,
    back_far,
    moe_send,
    moe_all,
    load_sem,
    send_sem,
    recv_sem,
    pair_sem,
    val_sem,
    near_sem,
    slot_sem,
    down_sem,
):
    far = (
        layer_in_far,
        rec_weight_far,
        key_weight_far,
        val_weight_far,
        out_weight_t_far,
        mix_gain_far,
        decay_down_t_far,
        rate_down_t_far,
        decay_up_far,
        rate_up_far,
        decay_base_far,
        rate_base_far,
        key_scale_far,
        group_gain_far,
        routes_t_far,
        gates_t_far,
        post_gain_far,
        ffn_gain_far,
        out_gain_far,
        state_far,
        expert_gate_far.at[0],
        expert_up_far.at[0],
        expert_down_far.at[0],
    )
    near = (
        layer_in,
        rec_weight,
        key_weight,
        val_weight,
        out_send,
        mix_gain,
        decay_down_t,
        rate_down_t,
        decay_up,
        rate_up,
        decay_base,
        rate_base,
        key_scale,
        group_gain,
        routes_t,
        gates_t,
        post_gain,
        ffn_gain,
        out_gain,
        state,
        w_gate,
        w_up,
        w_down,
    )
    loads = [pltpu.make_async_copy(a, b, load_sem.at[n]) for n, (a, b) in enumerate(zip(far, near))]
    first_big = len(loads) - 4
    seqs, width = layer_in.shape
    heads = state.shape[1]
    plane = heads
    n_z = n_ep // plane
    quarter = width // n_tp
    tiles = quarter // LANES
    slab = CAP * tiles
    rows = seqs * heads
    depth = rec_weight.shape[0]
    out_cols = out_send.shape[0]

    for load in loads[:5]:
        load.start()

    me = lax.axis_index("ep")
    mine = lax.axis_index("tp")
    member = lax.rem(me, plane)
    base = me - member

    def member_at(step):
        return lax.rem(member + step, plane)

    def z_at(step):
        return lax.rem(me + step * plane, n_ep)

    def tp_at(step):
        return lax.rem(mine + step, n_tp)

    def send(src, dst, phase, ep, tp, sem=None):
        pltpu.make_async_remote_copy(
            src_ref=src,
            dst_ref=dst,
            send_sem=send_sem.at[phase],
            recv_sem=recv_sem.at[phase] if sem is None else sem,
            device_id={"ep": ep, "tp": tp},
            device_id_type=MESH,
        ).start()

    def keep(src, dst, sem):
        pltpu.make_async_copy(src, dst, sem).start()

    def arrive(buffer, sem):
        pltpu.make_async_copy(buffer, buffer, sem).wait()

    def sent(buffer, phase):
        pltpu.make_async_copy(buffer, buffer, send_sem.at[phase]).wait()

    def loop(start, stop, body):
        def step(i, carry):
            body(i)
            return carry

        lax.fori_loop(start, stop, step, 0)

    barrier = pltpu.get_barrier_semaphore()

    def others(body):
        for k in range(n_z):
            away = n_z // 2 + (k + 1) // 2 * (1 if k % 2 else -1)
            first = lax.rem(base + away % n_z * plane, n_ep)
            loop(
                0 if away % n_z else 1,
                plane,
                lambda i, first=first, away=away: body(first + member_at(i), away),
            )

    def greet(to, away):
        pl.semaphore_signal(barrier, inc=1, device_id={"ep": to, "tp": mine}, device_id_type=MESH)

    others(greet)

    def greet_plane(i):
        pl.semaphore_signal(
            barrier,
            inc=1,
            device_id={"ep": base + member_at(lax.rem(i, plane)), "tp": tp_at(i // plane)},
            device_id_type=MESH,
        )

    loop(plane, plane * n_tp, greet_plane)

    for load in loads[5:first_big]:
        load.start()
    for load in loads[:5]:
        load.wait()
    for h in range(heads):
        cut = slice(h * HEAD_DIM, (h + 1) * HEAD_DIM)
        pair_send[h] = jnp.concatenate([rec_weight[:, cut], key_weight[:, cut]], axis=1)
        val_send[h] = jnp.concatenate(
            [val_weight[: depth // 2, cut], val_weight[depth // 2 :, cut]], axis=1
        )
    for load in loads[first_big:]:
        load.start()
    for load in loads[5:first_big]:
        load.wait()
    pl.semaphore_wait(barrier, n_ep - 1 + plane * (n_tp - 1))

    keep(pair_send.at[member], pair_all.at[me], pair_sem.at[0])
    keep(val_send.at[member], val_all.at[me], val_sem.at[0])
    pair_wave = (pair_send, pair_all, 1, pair_sem)
    val_wave = (val_send, val_all, 15, val_sem)

    def send_wave(wave, away):
        src, dst, phase, sem = wave
        first = lax.rem(base + away % n_z * plane, n_ep)

        def one(i):
            to = member_at(i)
            send(src.at[to], dst.at[me], phase, first + to, mine, sem.at[-away % n_z])

        loop(0 if away else 1, plane, one)

    for away in (2, -2):
        send_wave(pair_wave, away)
    chip, core = member // 2, lax.rem(member, 2)
    keep(layer_in, rows_all.at[chip, core], recv_sem.at[0])

    def send_rows(i):
        send(layer_in, rows_all.at[chip, core], 0, base + member_at(2 * i), mine)

    loop(1, plane // 2, send_rows)
    for away in (1, -1, 0):
        send_wave(pair_wave, away)
    for away in (2, -2):
        send_wave(val_wave, away)
    z_me = me // plane

    own_normed = rms_scale(layer_in[...].astype(F32), mix_gain[...]).astype(BF16)
    decay_hidden = jnp.tanh(dot_t(own_normed, decay_down_t[...])).astype(BF16)
    rate_hidden = dot_t(own_normed, rate_down_t[...]).astype(BF16)
    decay_sig = jax.nn.sigmoid(decay_base[...] + dot(decay_hidden, decay_up[...]))
    decay = jnp.exp(-jnp.exp(jnp.full((), -0.5, F32)) * decay_sig)
    rate = jax.nn.sigmoid(rate_base[...] + dot(rate_hidden, rate_up[...]))
    for h in range(heads):
        cut = slice(h * HEAD_DIM, (h + 1) * HEAD_DIM)
        decay_rows[h * seqs : (h + 1) * seqs, :] = decay[:, cut]
        rate_rows[h * seqs : (h + 1) * seqs, :] = rate[:, cut]
        by_head[0, h : h + 1, :] = key_scale[:, cut]
        by_head[1, h : h + 1, :] = group_gain[:, cut]

    top = routes_t.shape[0]
    named_t = jnp.zeros((n_ep, seqs), F32)
    weight_t = jnp.zeros((n_ep, seqs), F32)
    for j in range(top):
        hit = iota((n_ep, seqs), 0) == routes_t[j : j + 1, :]
        named_t += jnp.where(hit, 1.0, 0.0)
        weight_t += jnp.where(hit, gates_t[j : j + 1, :], 0.0)
    before_t = dot(named_t.astype(BF16), one_hot(iota((seqs, seqs), 0) < iota((seqs, seqs), 1)))
    eye = one_hot(iota((seqs, seqs), 0) == iota((seqs, seqs), 1))
    combine = []
    for s in range(CAP):
        high, low = split(jnp.where(before_t == float(s), weight_t, 0.0))
        combine.append((dot_t(eye, high).astype(BF16), dot_t(eye, low).astype(BF16)))
    per = WIDE // HEAD_DIM

    def tables(i):
        block = pl.ds(pl.multiple_of(i * WIDE, WIDE), WIDE)
        pick_all[:, block] = one_hot(
            iota((HEAD_DIM, WIDE), 0) == i * per + iota((HEAD_DIM, WIDE), 1) // HEAD_DIM
        )
        gather_all[block, :] = one_hot(
            iota((WIDE, HEAD_DIM), 1) == i * per + iota((WIDE, HEAD_DIM), 0) // HEAD_DIM
        )

    loop(0, HEAD_DIM // per, tables)

    def plane_of(buffer, away):
        at = lax.rem(base + away % n_z * plane, n_ep)
        return at, buffer.at[pl.ds(at, plane)]

    half = plane // 2

    def forward(wave):
        _, buffer, phase, sem = wave
        for away in (-2, 2):
            at, blocks = plane_of(buffer, away)
            arrive(blocks, sem.at[away % n_z])
            side = -away // 2
            to = lax.rem(base + side % n_z * plane, n_ep) + member
            send(blocks, blocks, phase, to, mine, sem.at[(away - side) % n_z])
            part = buffer.at[pl.ds(at + (0 if side > 0 else half), half)]
            to = lax.rem(base + 2 * side % n_z * plane, n_ep) + member
            send(part, part, phase, to, mine, sem.at[(away - 2 * side) % n_z])

    def arrive_wave(wave):
        _, buffer, _, sem = wave
        for away in (0, 1, -1, 3, -3, 4):
            arrive(plane_of(buffer, away)[1], sem.at[away % n_z])

    forward(pair_wave)
    for away in (1, -1, 0):
        send_wave(val_wave, away)
    arrive(rows_all.at[:, core], recv_sem.at[0])
    sibling = me + 1 - 2 * core
    send(rows_all.at[:, core], rows_all.at[:, core], 13, sibling, mine)
    forward(val_wave)

    arrive(rows_all.at[:, 1 - core], recv_sem.at[13])

    def norm_rows(i):
        values = rms_scale(rows_all[i // 2, lax.rem(i, 2)].astype(F32), mix_gain[...]).astype(BF16)
        normed_all[pl.ds(pl.multiple_of(i * seqs, seqs), seqs), :] = values

    loop(0, plane, norm_rows)

    turn = one_hot(
        iota((rows, rows), 1)
        == lax.rem(iota((rows, rows), 0), heads) * seqs + iota((rows, rows), 0) // heads
    )
    turn_back = one_hot(
        iota((rows, rows), 1)
        == lax.rem(iota((rows, rows), 0), seqs) * heads + iota((rows, rows), 0) // seqs
    )
    decay_high, decay_low = split(decay_rows[...])
    rate_high, rate_low = split(rate_rows[...])
    turned = dot(turn, jnp.concatenate([decay_high, decay_low, rate_high, rate_low], axis=1))
    decay = turned[:, :HEAD_DIM] + turned[:, HEAD_DIM : 2 * HEAD_DIM]
    rate = turned[:, 2 * HEAD_DIM : 3 * HEAD_DIM] + turned[:, 3 * HEAD_DIM :]

    arrive_wave(pair_wave)
    normed = normed_all[...]
    pair_sum = dot(normed, pair_all[...].reshape(n_ep * depth, 2 * HEAD_DIM))
    pair_out[...] = pair_sum.astype(BF16).reshape(plane, seqs, 2 * HEAD_DIM)

    def share(src, dst, phase):
        keep(src.at[member], dst.at[member], recv_sem.at[phase])

        def one(i):
            to = member_at(i)
            send(src.at[to], dst.at[member], phase, base + to, mine)

        loop(1, plane, one)

    share(pair_out, pair_in, 3)
    keep(out_send, out_all.at[z_me], recv_sem.at[2])

    def send_out(i):
        send(out_send, out_all.at[z_me], 2, z_at(i), mine)

    loop(1, n_z, send_out)

    arrive_wave(val_wave)
    vals = val_all[...]
    vals = jnp.concatenate([vals, vals], axis=1).reshape(n_ep * depth, 2 * HEAD_DIM)
    spread = (n_ep * depth, 2 * HEAD_DIM)
    first = lax.rem(iota(spread, 0), depth) < depth // 2
    vals = jnp.where(first == (iota(spread, 1) < HEAD_DIM), vals.astype(F32), 0.0).astype(BF16)
    val_sum = dot(normed, vals)
    val_sum = val_sum[:, :HEAD_DIM] + val_sum[:, HEAD_DIM:]
    val_sum = jnp.concatenate([val_sum, jnp.zeros_like(val_sum)], axis=1)
    val_out[...] = val_sum.astype(BF16).reshape(plane, seqs, 2 * HEAD_DIM)
    share(val_out, val_in, 16)

    arrive(pair_in, recv_sem.at[3])
    pair = dot(turn, pair_in[...].reshape(rows, 2 * HEAD_DIM))
    rec = pair[:, :HEAD_DIM]
    key = pair[:, HEAD_DIM:]

    def of_heads(n):
        return jnp.broadcast_to(by_head[n][None], (seqs, heads, HEAD_DIM)).reshape(rows, HEAD_DIM)

    scaled = key * of_heads(0)
    unit = scaled * lax.rsqrt(jnp.sum(scaled * scaled, axis=-1, keepdims=True) + norm_eps)

    def wide(a):
        return jnp.concatenate([a] * (WIDE // HEAD_DIM), axis=1)

    unit_w, read_w = wide(unit), wide(decay * rec)
    loads[first_big].wait()

    def sums(i, totals):
        for k in range(4):
            block = pl.ds(pl.multiple_of((i * 4 + k) * WIDE, WIDE), WIDE)
            old = state[:, :, block].reshape(rows, WIDE)
            stacked = jnp.concatenate(split(old * unit_w) + split(old * read_w), axis=0)
            totals += dot(stacked, gather_all[block, :])
        return totals

    totals = lax.fori_loop(0, HEAD_DIM // per // 4, sums, jnp.zeros((4 * rows, HEAD_DIM), F32))
    along = totals[:rows] + totals[rows : 2 * rows]
    along_read = jnp.sum(unit * rate * rec, axis=-1, keepdims=True)
    val_read = jnp.sum(key * rate * rec, axis=-1, keepdims=True)
    arrive(val_in, recv_sem.at[16])
    val = dot(turn, val_in[...].reshape(rows, 2 * HEAD_DIM))[:, :HEAD_DIM].astype(BF16)
    readout = totals[2 * rows : 3 * rows] + totals[3 * rows :] - along * along_read + val.astype(F32) * val_read
    centred = readout - jnp.mean(readout, axis=-1, keepdims=True)
    normed_out = centred * lax.rsqrt(jnp.mean(centred * centred, axis=-1, keepdims=True) + group_eps)
    normed_out = dot(turn_back, (normed_out * of_heads(1)).astype(BF16)).astype(BF16)
    for h in range(heads):
        read_send[:, h * HEAD_DIM : (h + 1) * HEAD_DIM] = normed_out[h * seqs : (h + 1) * seqs, :]
    keep(read_send, read_all.at[member], recv_sem.at[4])

    def send_read(i):
        send(read_send, read_all.at[member], 4, base + member_at(i), mine)

    loop(1, plane, send_read)

    decay_w, unit_rate, key_rate = wide(decay), wide(unit * rate), wide(key * rate)
    along_high, along_low = split(along)
    spread_rows = jnp.concatenate([along_high, along_low, val], axis=0)

    def update(i):
        for k in range(2):
            block = pl.ds(pl.multiple_of((i * 2 + k) * WIDE, WIDE), WIDE)
            wider = dot(spread_rows, pick_all[:, block])
            old = state[:, :, block].reshape(rows, WIDE)
            new = old * decay_w - (wider[:rows] + wider[rows : 2 * rows]) * unit_rate
            new += wider[2 * rows :] * key_rate
            new_state[:, :, block] = new.reshape(seqs, heads, WIDE)

    loop(0, HEAD_DIM // per // 2, update)

    arrive(out_all, recv_sem.at[2])
    arrive(read_all, recv_sem.at[4])
    part = dot_t(
        read_all[...].reshape(plane * seqs, quarter), out_all[...].reshape(n_z * out_cols, quarter)
    )
    part_send[...] = part.astype(BF16).reshape(plane, seqs, n_z * out_cols)
    keep(part_send.at[member], part_all.at[mine * plane + member], recv_sem.at[5])

    def send_part(i, step):
        to = member_at(i)
        send(part_send.at[to], part_all.at[mine * plane + member], 5, base + to, tp_at(step))

    for step in (2, 1, n_tp - 1):
        loop(plane // 2, plane + plane // 2, functools.partial(send_part, step=step))
    loop(1, plane, functools.partial(send_part, step=0))

    arrive(part_all, recv_sem.at[5])
    for g in range(plane):
        total = part_all[g].astype(F32)
        for t in range(1, n_tp):
            total += part_all[t * plane + g].astype(F32)
        for z in range(n_z):
            at = (z * plane + g) * out_cols
            mix_rows[:, at : at + out_cols] = total[:, z * out_cols : (z + 1) * out_cols]
    middle = (layer_in[...].astype(F32) + rms_scale(mix_rows[...], post_gain[...])).astype(BF16)
    mix_rows[...] = middle.astype(F32)
    ffn_in = rms_scale(mix_rows[...], ffn_gain[...])

    mix_rows[...] = ffn_in
    opposite = tp_at(n_tp // 2)

    def to_slabs(values, dst):
        for s in range(CAP):
            for t in range(tiles):
                wide_rows[pl.ds(s * tiles + t, n_ep, stride=slab), :] = values[s][:, t * LANES : (t + 1) * LANES]
        dst[...] = wide_rows[...].astype(BF16).reshape(n_ep, slab, LANES)

    def to_everyone(src, dst, phase, sems=None):
        def sem_of(away):
            return recv_sem.at[phase] if sems is None else sems.at[-away % n_z]

        keep(src.at[me], dst.at[me], sem_of(0))
        others(lambda to, away: send(src.at[to], dst.at[me], phase, to, mine, sem_of(away)))

    for at, src, dst, phase, sems in (
        (mine, slot_send, slot_here, 6, near_sem),
        (opposite, slot_far_send, slot_far, 11, None),
    ):
        cut = mix_rows[:, pl.ds(pl.multiple_of(at * quarter, quarter), quarter)].astype(BF16)
        to_slabs(
            [dot(jnp.where(before_t == float(s), named_t, 0.0).astype(BF16), cut) for s in range(CAP)], src
        )
        to_everyone(src, dst, phase, sems)
    mix_rows[...] = middle.astype(F32)

    sides = (1, n_tp - 1)
    for away in (0, 1, -1, 2, -2, 3, -3, 4):
        at, blocks = plane_of(slot_here, away)
        arrive(blocks, near_sem.at[away % n_z])
        for step in sides:
            send(blocks, slot_all.at[mine, pl.ds(at, plane)], 7, me, tp_at(step), slot_sem.at[mine])
    loads[first_big + 1].wait()
    loads[first_big + 2].wait()

    def from_slabs(source):
        wide_rows[...] = source.astype(F32).reshape(n_ep * slab, LANES)
        return [
            [wide_rows[pl.ds(s * tiles + t, n_ep, stride=slab), :] for t in range(tiles)]
            for s in range(CAP)
        ]

    gate = up = None
    for step in (0, n_tp // 2) + sides:
        at = tp_at(step)
        if step == 0:
            source = slot_here[...]
        elif step == n_tp // 2:
            arrive(slot_far, recv_sem.at[11])
            source = slot_far[...]
        else:
            arrive(slot_all.at[at], slot_sem.at[at])
            source = slot_all[at]
        part = jnp.concatenate(
            [jnp.concatenate(p, axis=1).reshape(n_z, 1, plane, quarter) for p in from_slabs(source)], axis=1
        )
        part = part.reshape(n_ep * CAP, quarter).astype(BF16)
        feats = pl.ds(pl.multiple_of(at * quarter, quarter), quarter)
        gate_part, up_part = dot(part, w_gate[feats, :]), dot(part, w_up[feats, :])
        gate = gate_part if gate is None else gate + gate_part
        up = up_part if up is None else up + up_part
    gate = jnp.minimum(gate, clamp_limit)
    up = jnp.clip(up, -clamp_limit, clamp_limit)
    hidden = ((up + 1.0) * gate * jax.nn.sigmoid(gate_alpha * gate)).astype(BF16)

    loads[first_big + 3].wait()

    def down(at):
        return dot(hidden, w_down[:, pl.ds(pl.multiple_of(at * quarter, quarter), quarter)]).astype(BF16)

    planes = [n_z // 2 + (k + 1) // 2 * (1 if k % 2 else -1) for k in range(n_z)]

    def block_of(away):
        at = lax.rem(base + away % n_z * plane, n_ep)
        return at, pl.ds(pl.multiple_of(at * CAP, plane * CAP), plane * CAP)

    for side, step in enumerate(sides):
        at = tp_at(step)
        down_send[at] = down(at)
        for away in planes:
            block = block_of(away)[1]
            send(
                down_send.at[at, block],
                down_all.at[mine, block],
                8,
                me,
                at,
                down_sem.at[side * n_z + away % n_z],
            )
    values = down(opposite).astype(F32).reshape(n_z, CAP, plane, quarter)
    to_slabs([values[:, s].reshape(n_ep, quarter) for s in range(CAP)], back_far_send)
    to_everyone(back_far_send, back_far, 12)
    down_all[mine] = down(mine)

    for away in planes:
        at, block = block_of(away)
        total = down_all[mine, block].astype(F32)
        for side, step in enumerate(sides):
            source = tp_at(n_tp - step)
            arrive(down_all.at[source, block], down_sem.at[side * n_z + away % n_z])
            total += down_all[source, block].astype(F32)
        for s in range(CAP):
            for t in range(tiles):
                wide_rows[pl.ds(at * slab + s * tiles + t, plane, stride=slab), :] = total[
                    s * plane : (s + 1) * plane, t * LANES : (t + 1) * LANES
                ]
        slabs = wide_rows[pl.ds(pl.multiple_of(at * slab, plane * slab), plane * slab), :]
        back_send[pl.ds(at, plane)] = slabs.astype(BF16).reshape(plane, slab, LANES)

        def send_back(i, at=at):
            to = at + member_at(i)
            send(back_send.at[to], back_all.at[me], 9, to, mine)

        if away % n_z == 0:
            keep(back_send.at[me], back_all.at[me], recv_sem.at[9])
        loop(0 if away % n_z else 1, plane, send_back)

    for n, (buffer, phase) in enumerate(((back_far, 12), (back_all, 9))):
        arrive(buffer, recv_sem.at[phase])
        moe = jnp.zeros((seqs, quarter), F32)
        for (high, low), p in zip(combine, from_slabs(buffer[...])):
            values = jnp.concatenate(p, axis=1).astype(BF16)
            moe += dot(high, values) + dot(low, values)
        moe_send[n] = moe.astype(BF16)
        last = 14 if n == 0 else 10
        keep(moe_send.at[n], moe_all.at[n, mine], recv_sem.at[last])
        for step in range(1, n_tp):
            send(moe_send.at[n], moe_all.at[n, mine], last, me, tp_at(step))
    arrive(moe_all.at[0], recv_sem.at[14])
    arrive(moe_all.at[1], recv_sem.at[10])
    moe = jnp.concatenate(
        [moe_all[1, t].astype(F32) + moe_all[0, (t + n_tp // 2) % n_tp].astype(F32) for t in range(n_tp)], axis=1
    )
    layer_out[...] = (mix_rows[...] + rms_scale(moe, out_gain[...])).astype(BF16)

    sent(rows_all.at[pl.ds(0, plane // 2 - 1), 0], 0)
    sent(rows_all.at[:, core], 13)
    sent(moe_all.at[0, pl.ds(0, n_tp - 1)], 14)
    sent(pair_all.at[pl.ds(0, n_ep - 1)], 1)
    sent(val_all.at[pl.ds(0, n_ep - 1)], 15)
    sent(out_all.at[pl.ds(0, n_z - 1)], 2)
    sent(slot_far.at[pl.ds(0, n_ep - 1)], 11)
    sent(back_far.at[pl.ds(0, n_ep - 1)], 12)
    sent(pair_in.at[pl.ds(0, plane - 1)], 3)
    sent(val_in.at[pl.ds(0, plane - 1)], 16)
    sent(read_all.at[pl.ds(0, plane - 1)], 4)
    sent(part_all.at[pl.ds(0, n_tp * plane - 1)], 5)
    sent(slot_here.at[pl.ds(0, n_ep - 1)], 6)
    sent(slot_all.at[pl.ds(0, 2)], 7)
    sent(down_all.at[pl.ds(0, 2)], 8)
    sent(back_all.at[pl.ds(0, n_ep - 1)], 9)
    sent(moe_all.at[1, pl.ds(0, n_tp - 1)], 10)


def local(n_ep, n_tp, *args):
    (
        layer_in,
        state_in,
        mix_gain,
        rec_weight,
        key_weight,
        val_weight,
        decay_down,
        decay_up,
        decay_base,
        rate_down,
        rate_up,
        rate_base,
        key_scale,
        group_gain,
        out_weight,
        post_gain,
        ffn_gain,
        routes,
        route_gates,
        expert_gate,
        expert_up,
        expert_down,
        out_gain,
    ) = args
    seqs, width = layer_in.shape
    heads = state_in.shape[1]
    plane = heads
    n_z = n_ep // plane
    quarter = width // n_tp
    slab = CAP * (quarter // LANES)
    depth = rec_weight.shape[0]
    out_cols = out_weight.shape[1]
    slots = CAP * n_ep
    state_lanes = state_in.shape[2]
    row = lambda a: a.reshape(1, -1)
    operands = (
        layer_in,
        rec_weight,
        key_weight,
        val_weight,
        out_weight.T,
        row(mix_gain),
        decay_down.T,
        rate_down.T,
        decay_up,
        rate_up,
        row(decay_base),
        row(rate_base),
        row(key_scale),
        row(group_gain),
        routes.T,
        route_gates.T,
        row(post_gain),
        row(ffn_gain),
        row(out_gain),
        state_in,
        expert_gate,
        expert_up,
        expert_down,
    )
    far = pl.BlockSpec(memory_space=pltpu.HBM)
    local_shapes = [a.shape[1:] if a.ndim == 3 and n >= len(operands) - 3 else a.shape for n, a in enumerate(operands)]
    scratch = [pltpu.VMEM(shape, a.dtype) for shape, a in zip(local_shapes, operands)]
    scratch += [
        pltpu.VMEM((plane, depth, 2 * HEAD_DIM), BF16),
        pltpu.VMEM((n_ep, depth, 2 * HEAD_DIM), BF16),
        pltpu.VMEM((plane, depth // 2, 2 * HEAD_DIM), BF16),
        pltpu.VMEM((n_ep, depth // 2, 2 * HEAD_DIM), BF16),
        pltpu.VMEM((n_z, out_cols, quarter), BF16),
        pltpu.VMEM((plane // 2, 2, seqs, width), BF16),
        pltpu.VMEM((plane * seqs, width), BF16),
        pltpu.VMEM((plane, seqs, 2 * HEAD_DIM), BF16),
        pltpu.VMEM((plane, seqs, 2 * HEAD_DIM), BF16),
        pltpu.VMEM((plane, seqs, 2 * HEAD_DIM), BF16),
        pltpu.VMEM((plane, seqs, 2 * HEAD_DIM), BF16),
        pltpu.VMEM((heads * seqs, HEAD_DIM), F32),
        pltpu.VMEM((heads * seqs, HEAD_DIM), F32),
        pltpu.VMEM((2, heads, HEAD_DIM), F32),
        pltpu.VMEM((HEAD_DIM * HEAD_DIM, HEAD_DIM), BF16),
        pltpu.VMEM((HEAD_DIM, HEAD_DIM * HEAD_DIM), BF16),
        pltpu.VMEM((seqs, quarter), BF16),
        pltpu.VMEM((plane, seqs, quarter), BF16),
        pltpu.VMEM((plane, seqs, n_z * out_cols), BF16),
        pltpu.VMEM((n_tp * plane, seqs, n_z * out_cols), BF16),
        pltpu.VMEM((seqs, width), F32),
        pltpu.VMEM((n_ep * slab, LANES), F32),
        pltpu.VMEM((n_ep, slab, LANES), BF16),
        pltpu.VMEM((n_ep, slab, LANES), BF16),
        pltpu.VMEM((n_ep, slab, LANES), BF16),
        pltpu.VMEM((n_ep, slab, LANES), BF16),
        pltpu.VMEM((n_tp, n_ep, slab, LANES), BF16),
        pltpu.VMEM((n_tp, slots, quarter), BF16),
        pltpu.VMEM((n_tp, slots, quarter), BF16),
        pltpu.VMEM((n_ep, slab, LANES), BF16),
        pltpu.VMEM((n_ep, slab, LANES), BF16),
        pltpu.VMEM((n_ep, slab, LANES), BF16),
        pltpu.VMEM((n_ep, slab, LANES), BF16),
        pltpu.VMEM((2, seqs, quarter), BF16),
        pltpu.VMEM((2, n_tp, seqs, quarter), BF16),
        pltpu.SemaphoreType.DMA((len(operands),)),
        pltpu.SemaphoreType.DMA((17,)),
        pltpu.SemaphoreType.DMA((17,)),
        pltpu.SemaphoreType.DMA((n_z,)),
        pltpu.SemaphoreType.DMA((n_z,)),
        pltpu.SemaphoreType.DMA((n_z,)),
        pltpu.SemaphoreType.DMA((n_tp,)),
        pltpu.SemaphoreType.DMA((2 * n_z,)),
    ]
    return pl.pallas_call(
        functools.partial(kernel, n_ep, n_tp),
        out_shape=(
            jax.ShapeDtypeStruct(layer_in.shape, BF16),
            jax.ShapeDtypeStruct((seqs, heads, state_lanes), F32),
        ),
        in_specs=[far] * len(operands),
        out_specs=[pl.BlockSpec(memory_space=pltpu.VMEM)] * 2,
        scratch_shapes=scratch,
        compiler_params=pltpu.CompilerParams(
            collective_id=0, has_side_effects=True, vmem_limit_bytes=32 * 1024 * 1024
        ),
    )(*[pltpu.with_memory_space_constraint(a, pltpu.HBM) for a in operands])


def solution(mesh):
    in_specs = (
        P("ep", None),
        P("ep", "tp", None),
        P(),
        P("ep", "tp"),
        P("ep", "tp"),
        P("ep", "tp"),
        P(),
        P(None, "tp"),
        P("tp"),
        P(),
        P(None, "tp"),
        P("tp"),
        P("tp"),
        P("tp"),
        P("tp", "ep"),
        P(),
        P(),
        P("ep", None),
        P("ep", None),
        P("ep", None, "tp"),
        P("ep", None, "tp"),
        P("ep", "tp", None),
        P(),
    )
    out_specs = (P("ep", None), P("ep", "tp", None))
    body = functools.partial(local, mesh.shape["ep"], mesh.shape["tp"])
    return jax.shard_map(body, mesh=mesh, in_specs=in_specs, out_specs=out_specs, check_vma=False)
```
